128 devices in a mesh: sp: 32 (over z, y, core), tp: 4 (over x).
Axes of the slice: x: 4, y: 4, z: 4, core: 2. Of those that a mesh axis runs over, the one named last changes fastest.
Arguments:
- resid_in: bfloat16 [12288, 2048], P('sp'), may hold values from -6 to 6
- cotangent: bfloat16 [12288, 2048], P('sp'), may hold values from -2 to 2
- norm_gain: float32 [2048], replicated, may hold values from 0.1 to 1.9
- routes: int32 [12288, 2], P('sp'), may hold values from 0 to 31, all different within a row; in each aligned block of 384 rows (0 to 383, 384 to 767, ...) at most 48 rows name the same one
- route_weights: float32 [12288, 2], P('sp'), may hold values from 0.1 to 1
- gate_weight: bfloat16 [32, 2048, 1024], P('sp', None, 'tp'), may hold values from -0.125 to 0.125
- up_weight: bfloat16 [32, 2048, 1024], P('sp', None, 'tp'), may hold values from -0.125 to 0.125
- down_weight: bfloat16 [32, 1024, 2048], P('sp', 'tp'), may hold values from -0.1875 to 0.1875
- out_weight: bfloat16 [2048, 1024], P(None, 'tp'), may hold values from -0.1875 to 0.1875
- gate_b: bfloat16 [12288, 1024], P('sp', 'tp'), may hold values from -6 to 6
- gate_c: bfloat16 [12288, 1024], P('sp', 'tp'), may hold values from -6 to 6
- values_u: bfloat16 [12288, 1024], P('sp', 'tp'), may hold values from -6 to 6
- taps: float32 [3, 1024], P(None, 'tp'), may hold values from -3.5 to 3.5
Outputs:
- grad_gate_weight: float32 [32, 2048, 1024], P('sp', None, 'tp')
- grad_up_weight: float32 [32, 2048, 1024], P('sp', None, 'tp')
- grad_down_weight: float32 [32, 1024, 2048], P('sp', 'tp')
- grad_resid: bfloat16 [12288, 2048], P('sp')
- grad_out_weight: float32 [2048, 1024], P('sp', 'tp')
- grad_gate_b: bfloat16 [12288, 1024], P('sp', 'tp')
- grad_gate_c: bfloat16 [12288, 1024], P('sp', 'tp')
- grad_values: bfloat16 [12288, 1024], P('sp', 'tp')
The draws below stay inside these ranges and needn't reach their ends.
Inputs may be any that keep to these rules, and one draw needn't show every extreme that they name: `routes`: A row's 2 experts differ. In the rows of one index of sp (384 tokens) no expert is named more than 48 times, a bound that some block reaches.
All inputs are finite; a program needn't handle non-finite values.
Results may differ from the reference program's by a relative error of at most 0.024.
Values may be sent and summed in bfloat16 or wider, within the bound.
A program may use at most 128 MiB of HBM per device.

```python
import math
import jax
import jax.numpy as jnp
import numpy as np
from jax import lax

D = 2048
SC = 1024
FF = 1024
TAPS = 3
TOP = 2
TOK_DEV = 384
EXPERTS = 32
CAP = 48
TOKENS = 12288
N_SP = 32
N_TP = 4


def with_spikes(entries, own_key, source, target, parts, factor):
    owner, partner = [(jnp.arange(entries.shape[axis_at]) // (entries.shape[axis_at] // parts)).reshape([-1 if axis == axis_at else 1 for axis in range(entries.ndim)]) for axis_at in (source, target)]
    chosen = jax.random.permutation(own_key, parts)[partner]
    strong = (owner == chosen) | (owner == (partner + parts // 2) % parts)
    return jnp.where(strong, factor * entries, entries)


def steps_of(key, shape, split, smallest, largest):
    factor_of, own = 1.0, jax.random.fold_in(key, 6)
    for position, blocks in split:
        draws = jnp.exp(jax.random.uniform(jax.random.fold_in(own, position), (blocks,), jnp.float32, smallest / len(split), largest / len(split)))
        factor_of = factor_of * jnp.repeat(draws, shape[position] // blocks).reshape([-1 if axis == position else 1 for axis in range(len(shape))])
    return factor_of


def deal_out(rng, own, number, rows, number_of, top, most, skew):
    sequence = jax.random.permutation(rng, number_of)
    heavy_load, common = shares(number_of, rows * top, most, skew, True), shares(number_of, rows * top, most, skew, False)
    places = jnp.arange(number_of)

    def named(tallies, rotation):
        used = int((tallies > 0).sum())
        fixed = max(1, used // 4)
        passed = fixed + (places - fixed + rotation * (used - fixed)) % max(1, number_of - fixed)
        return jnp.zeros((number_of,), jnp.int32).at[sequence[jnp.where(places < fixed, places, passed)]].set(jnp.asarray(tallies, jnp.int32))

    tallies = jnp.where(number % 4 == 0, named(heavy_load, number // 4), named(common, number - number // 4 - 1))
    mixed = jax.random.permutation(jax.random.fold_in(own, 3), number_of)
    source_of, receiver = mixed[0:number_of // 2 * 2:2], mixed[1:number_of // 2 * 2:2]
    room = jnp.minimum(tallies[source_of] - 1, most - tallies[receiver]) // 2
    room = jnp.where((source_of == sequence[0]) | (receiver == sequence[0]) | (tallies[receiver] == 0), 0, jnp.maximum(room, 0))
    passed = jax.random.randint(jax.random.fold_in(own, 4), (number_of // 2,), 0, 1 << 20) % (room + 1)
    tallies = tallies.at[source_of].add(-passed).at[receiver].add(passed)
    items = jnp.searchsorted(jnp.cumsum(tallies), jnp.arange(rows * top), side="right").astype(jnp.int32)
    listing = items.reshape(top, rows).T
    listing = listing[jax.random.permutation(jax.random.fold_in(own, 1), rows)]
    rotation = jax.random.randint(jax.random.fold_in(own, 2), (rows, 1), 0, top)
    return jnp.take_along_axis(listing, (jnp.arange(top)[None, :] + rotation) % top, axis=1)


def shares(number_of, total, reach, slope, full):
    portions = [(1 << 20) // math.isqrt(grade ** slope) + 1 for grade in range(1, number_of + 1)]
    largest = reach if full else min(reach, max(-(-total // number_of), total * portions[0] // sum(portions)))
    least = 1 if total - largest >= number_of - 1 else 0
    given, surplus = [largest] + [least] * (number_of - 1), total - largest - least * (number_of - 1)
    while surplus > 0:
        free = [i for i in range(1, number_of) if given[i] < largest] or [i for i in range(1, number_of) if given[i] < reach]
        pool, remaining = sum([portions[i] for i in free]), surplus
        for i in free:
            more = min(reach - given[i], max(1, remaining * portions[i] // pool), surplus)
            given[i] = given[i] + more
            surplus = surplus - more
    return np.array(given)


def gaussian(stream_key, extent, scale, reach, cuts=(), held_as=jnp.bfloat16):
    result = jax.random.normal(stream_key, extent, jnp.float32) * scale
    if len(cuts) > 0:
        result = steps_of(stream_key, extent, cuts, -0.22, 0.18) * result
    return jnp.clip(result, min=-reach, max=reach).astype(held_as)


def bell_draw_with(key, dims, spread, reach, pieces, heavy, held_as=jnp.bfloat16):
    drawn = spread * jax.random.normal(key, dims, jnp.float32)
    if pieces:
        drawn = drawn * steps_of(key, dims, pieces, -0.22, 0.18)
    return jnp.clip(with_spikes(drawn, jax.random.fold_in(key, 3), *heavy), -reach, reach).astype(held_as)


def setup_inputs(seed: int = 0) -> dict:
    arg_keys = jax.random.split(jax.random.key(seed), 14)
    resid_in = gaussian(arg_keys[0], (TOKENS, D), 1.0, 6.0, ((0, 32),))
    cotangent = bell_draw_with(arg_keys[1], (TOKENS, D), 0.25, 2.0, ((0, 32),), (0, 1, 32, 2.75))
    norm_gain = jnp.clip(1.0 + 0.18 * jax.random.normal(arg_keys[2], (D,), jnp.float32), 0.1, 1.9)
    routes_keys = jax.random.split(jax.random.fold_in(arg_keys[3], 1), TOKENS // TOK_DEV)
    routes_turns = jax.random.permutation(jax.random.fold_in(arg_keys[3], 3), TOKENS // TOK_DEV)
    routes = jax.vmap(lambda own, number: deal_out(jax.random.fold_in(arg_keys[3], 2), own, number, TOK_DEV, EXPERTS, TOP, CAP, 1))(routes_keys, routes_turns).reshape((TOKENS, TOP))
    route_weights = jnp.clip(0.1 + 0.9 * jax.random.uniform(arg_keys[4], (TOKENS, TOP), jnp.float32) ** steps_of(arg_keys[4], (TOKENS, TOP), ((0, 32),), -0.2, 0.2), 0.1, 1.0)
    gate_weight = gaussian(arg_keys[5], (EXPERTS, D, FF), D ** -0.5, 0.125, ((0, 32), (2, 4)))
    up_weight = gaussian(arg_keys[6], (EXPERTS, D, FF), D ** -0.5, 0.125, ((0, 32), (2, 4)))
    down_weight = gaussian(arg_keys[7], (EXPERTS, FF, D), FF ** -0.5, 0.1875, ((0, 32), (1, 4)))
    out_weight = gaussian(arg_keys[8], (D, SC), SC ** -0.5, 0.1875, ((1, 4),))
    gate_b = gaussian(arg_keys[9], (TOKENS, SC), 1.0, 6.0, ((0, 32), (1, 4)))
    gate_c = gaussian(arg_keys[10], (TOKENS, SC), 1.0, 6.0, ((0, 32), (1, 4)))
    values_u = gaussian(arg_keys[11], (TOKENS, SC), 1.0, 6.0, ((0, 32), (1, 4)))
    taps = gaussian(arg_keys[12], (TAPS, SC), TAPS ** -0.5, 3.5, ((1, 4),), jnp.float32)
    return dict(resid_in=resid_in, cotangent=cotangent, norm_gain=norm_gain, routes=routes, route_weights=route_weights, gate_weight=gate_weight, up_weight=up_weight, down_weight=down_weight, out_weight=out_weight, gate_b=gate_b, gate_c=gate_c, values_u=values_u, taps=taps)


norm_eps = 1e-06

def expert_pass(entry_rows, entry_cots, entry_weights, gate_mat, up_mat, down_mat):
    f32 = jnp.float32
    bf16 = jnp.bfloat16
    gate_pre = jnp.dot(entry_rows, gate_mat, preferred_element_type=f32)
    up_pre = jnp.dot(entry_rows, up_mat, preferred_element_type=f32)
    logistic = jax.nn.sigmoid(gate_pre)
    activated = gate_pre * logistic
    hidden = (activated * up_pre * entry_weights[:, None]).astype(bf16)
    grad_down = jnp.dot(hidden.T, entry_cots, preferred_element_type=f32)
    dhidden = jnp.dot(entry_cots, down_mat.T, preferred_element_type=f32) * entry_weights[:, None]
    dgate = (dhidden * up_pre * logistic * (1.0 + gate_pre * (1.0 - logistic))).astype(bf16)
    dup = (dhidden * activated).astype(bf16)
    grad_gate = jnp.dot(entry_rows.T, dgate, preferred_element_type=f32)
    grad_up = jnp.dot(entry_rows.T, dup, preferred_element_type=f32)
    quarter = gate_mat.shape[1] // N_TP
    summed = jnp.zeros((entry_rows.shape[0], entry_rows.shape[1]), f32)
    for lane_index in range(N_TP):
        lower = lane_index * quarter
        upper = lower + quarter
        partial_sum = jnp.dot(dgate[:, lower:upper], gate_mat[:, lower:upper].T, preferred_element_type=f32) + jnp.dot(dup[:, lower:upper], up_mat[:, lower:upper].T, preferred_element_type=f32)
        summed = summed + lax.optimization_barrier(partial_sum.astype(bf16)).astype(f32)
    return (grad_gate, grad_up, grad_down, summed.astype(bf16))

def reference(resid_in, cotangent, norm_gain, routes, route_weights, gate_weight, up_weight, down_weight, out_weight, gate_b, gate_c, values_u, taps):
    f32 = jnp.float32
    bf16 = jnp.bfloat16
    token_total = resid_in.shape[0]
    resid_wide = resid_in.astype(f32)
    inv_rms = lax.rsqrt(lax.optimization_barrier(jnp.mean(resid_wide * resid_wide, axis=1, keepdims=True)) + norm_eps)
    normed = (resid_wide * inv_rms * norm_gain).astype(bf16)
    flat_routes = routes.reshape(-1).astype(jnp.int32)
    flat_weights = route_weights.reshape(-1)
    slot_total = N_SP * CAP

    def one_expert(expert_id):
        chosen = flat_routes == expert_id
        found = jnp.nonzero(chosen, size=slot_total, fill_value=0)[0].astype(jnp.int32)
        how_many = jnp.sum(chosen.astype(jnp.int32))
        is_valid = jnp.arange(slot_total, dtype=jnp.int32) < how_many
        owners = found // 2
        entry_weights = jnp.where(is_valid, flat_weights[found], jnp.zeros((), f32))
        grads = expert_pass(normed[owners], cotangent[owners], entry_weights, gate_weight[expert_id], up_weight[expert_id], down_weight[expert_id])
        targets = jnp.where(is_valid, found, 2 * token_total).astype(jnp.int32)
        return (grads[0], grads[1], grads[2], grads[3], targets)
    grad_gate_weight, grad_up_weight, grad_down_weight, slot_rows, targets = lax.map(one_expert, jnp.arange(EXPERTS, dtype=jnp.int32))
    slot_grads = jnp.zeros((2 * token_total + 1, D), f32).at[targets.reshape(-1)].add(slot_rows.reshape(-1, D).astype(f32))
    paired = slot_grads[:2 * token_total].reshape(token_total, 2, D)
    dnormed = paired[:, 0] + paired[:, 1]
    scaled = dnormed * norm_gain
    resid_grad = cotangent.astype(f32) + inv_rms * scaled - resid_wide * inv_rms ** 3 * lax.optimization_barrier(jnp.mean(scaled * resid_wide, axis=1, keepdims=True))
    grad_resid = resid_grad.astype(bf16)
    mixed = gate_c.astype(f32) * values_u.astype(f32)
    padded = jnp.pad(mixed, ((2, 0), (0, 0)))
    conv = taps[0] * padded[:-2] + taps[1] * padded[1:-1] + taps[2] * padded[2:]
    merged = (gate_b.astype(f32) * conv).astype(bf16)
    grad_out_weight = jnp.dot(grad_resid.T, merged, preferred_element_type=f32)
    dmerged = jnp.dot(grad_resid, out_weight, preferred_element_type=f32)
    grad_gate_b = (dmerged * conv).astype(bf16)
    dconv = dmerged * gate_b.astype(f32)
    padded_grad = jnp.pad(dconv, ((0, 2), (0, 0)))
    dmixed = taps[2] * padded_grad[:-2] + taps[1] * padded_grad[1:-1] + taps[0] * padded_grad[2:]
    grad_gate_c = (dmixed * values_u.astype(f32)).astype(bf16)
    grad_values = (dmixed * gate_c.astype(f32)).astype(bf16)
    return (grad_gate_weight, grad_up_weight, grad_down_weight, grad_resid, grad_out_weight, grad_gate_b, grad_gate_c, grad_values)
```

```python
import jax
import jax.numpy as jnp
from jax import lax
from jax.experimental import pallas as pl
from jax.experimental.pallas import tpu as pltpu
from jax.sharding import PartitionSpec as P

norm_eps = 1e-06


def passed_along(array, axis, by):
    size = lax.axis_size(axis)
    pairs = [(i, i + by) for i in range(size) if 0 <= i + by < size]
    return lax.ppermute(array, axis, pairs)


def cut_along(array, dim, size):
    before, after = (array.shape[:dim], array.shape[dim + 1 :])
    return jnp.moveaxis(array.reshape(*before, size, -1, *after), dim, 0)


def sum_at_owner(array, axis, dim):
    size = lax.axis_size(axis)
    tiles = lax.all_to_all(cut_along(array, dim, size), axis, 0, 0, tiled=True)
    return jnp.sum(tiles.astype(jnp.float32), axis=0)


MESH = pl.DeviceIdType.MESH
BF16 = jnp.bfloat16
F32 = jnp.float32
SLOTS = 48


def offsets(k):
    m = 7 * k
    return (m // 8) % 4, (m // 2) % 4, m % 2


def moved(s, k, sign):
    z, y, c = s // 8, (s // 2) % 4, s % 2
    dz, dy, dc = offsets(k)
    z = lax.rem(z + 4 + sign * dz, 4)
    y = lax.rem(y + 4 + sign * dy, 4)
    return (z * 4 + y) * 2 + lax.rem(c + dc, 2)


def greet_all(s, x, near):
    barrier = pltpu.get_barrier_semaphore()

    def greet(k, carry):
        pl.semaphore_signal(
            barrier, inc=1, device_id={"sp": moved(s, k, 1), "tp": x}, device_id_type=MESH
        )
        return carry

    lax.fori_loop(1, 32, greet, 0)
    for lane in near:
        pl.semaphore_signal(barrier, inc=1, device_id={"sp": s, "tp": lane}, device_id_type=MESH)
    pl.semaphore_wait(barrier, 31 + len(near))


def dispatch_kernel(packed, both, far_send, far_recv, near_send, near_recv, own_sem):
    s, x = lax.axis_index("sp"), lax.axis_index("tp")
    kind = lax.rem(x, 2)
    half = packed.shape[2] // 2
    sides = (lax.rem(x + 1, 4), lax.rem(x + 3, 4))
    greet_all(s, x, sides)

    def far(k):
        peer = moved(s, k, 1)
        return pltpu.make_async_remote_copy(
            src_ref=packed.at[peer],
            dst_ref=both.at[kind, s],
            send_sem=far_send.at[k],
            recv_sem=far_recv.at[k],
            device_id={"sp": peer, "tp": x},
            device_id_type=MESH,
        )

    def near(h, k, own=False):
        source = s if own else moved(s, k, -1)
        cols = pl.ds(h * half, half)
        return pltpu.make_async_remote_copy(
            src_ref=packed.at[source, :, cols] if own else both.at[kind, source, :, cols],
            dst_ref=both.at[kind, source, :, cols],
            send_sem=near_send.at[h, k],
            recv_sem=near_recv.at[h, k],
            device_id={"sp": s, "tp": sides[h]},
            device_id_type=MESH,
        )

    keep = pltpu.make_async_copy(packed.at[s], both.at[kind, s], own_sem)

    def go(k, carry):
        far(k).start()
        return carry

    lax.fori_loop(1, 32, go, 0)
    keep.start()
    for h in range(2):
        near(h, 0, True).start()

    def forward(k, carry):
        far(k).wait_recv()
        for h in range(2):
            near(h, k).start()
        return carry

    lax.fori_loop(1, 32, forward, 0)
    keep.wait()
    for h in range(2):
        near(h, 0, True).wait()

    def finish(k, carry):
        far(k).wait_send()
        for h in range(2):
            near(h, k).wait()
        return carry

    lax.fori_loop(1, 32, finish, 0)


def dispatch(packed):
    spec = pl.BlockSpec(memory_space=pl.ANY)
    return pl.pallas_call(
        dispatch_kernel,
        out_shape=jax.ShapeDtypeStruct((2,) + packed.shape, BF16),
        in_specs=[spec],
        out_specs=spec,
        scratch_shapes=[
            pltpu.SemaphoreType.DMA((32,)),
            pltpu.SemaphoreType.DMA((32,)),
            pltpu.SemaphoreType.DMA((2, 32)),
            pltpu.SemaphoreType.DMA((2, 32)),
            pltpu.SemaphoreType.DMA,
        ],
        compiler_params=pltpu.CompilerParams(collective_id=0, has_side_effects=True),
    )(packed)


def expert_pass(entry_rows, entry_cots, gate_mat, up_mat, down_mat):
    f32 = jnp.float32
    bf16 = jnp.bfloat16
    gate_pre = jnp.dot(entry_rows, gate_mat, preferred_element_type=f32)
    up_pre = jnp.dot(entry_rows, up_mat, preferred_element_type=f32)
    logistic = jax.nn.sigmoid(gate_pre)
    activated = gate_pre * logistic
    hidden = (activated * up_pre).astype(bf16)
    grad_down = jnp.einsum("rf,rd->fd", hidden, entry_cots, preferred_element_type=f32)
    dhidden = jnp.einsum("rd,fd->rf", entry_cots, down_mat, preferred_element_type=f32)
    dgate = (dhidden * up_pre * logistic * (1.0 + gate_pre * (1.0 - logistic))).astype(bf16)
    dup = (dhidden * activated).astype(bf16)
    grad_gate = jnp.einsum("rd,rf->df", entry_rows, dgate, preferred_element_type=f32)
    grad_up = jnp.einsum("rd,rf->df", entry_rows, dup, preferred_element_type=f32)
    partial_sum = jnp.einsum("rf,df->rd", dgate, gate_mat, preferred_element_type=f32) + jnp.einsum(
        "rf,df->rd", dup, up_mat, preferred_element_type=f32
    )
    return (grad_gate, grad_up, grad_down, partial_sum)


def on_device(
    resid_in,
    cotangent,
    norm_gain,
    routes,
    route_weights,
    gate_weight,
    up_weight,
    down_weight,
    out_weight,
    gate_b,
    gate_c,
    values_u,
    taps,
):
    f32 = jnp.float32
    bf16 = jnp.bfloat16
    token_count, model_width = resid_in.shape
    groups = lax.axis_size("sp")
    lanes = lax.axis_size("tp")
    local_experts = gate_weight.shape[0]
    expert_total = local_experts * groups
    capacity = 4 * token_count // expert_total
    slot_span = local_experts * capacity
    resid_wide = resid_in.astype(f32)
    inv_rms = lax.rsqrt(jnp.mean(resid_wide * resid_wide, axis=1, keepdims=True) + norm_eps)
    normed = (resid_wide * inv_rms * norm_gain).astype(bf16)
    mixed = gate_c.astype(f32) * values_u.astype(f32)
    earlier = passed_along(mixed[-2:], "sp", 1)
    experts = jnp.arange(expert_total, dtype=jnp.int32)[:, None]
    first, second = (routes[:, 0] == experts).astype(f32), (routes[:, 1] == experts).astype(f32)
    earlier_rows = jnp.arange(token_count)[:, None] < jnp.arange(token_count)[None, :]
    ahead = jnp.dot(
        (first + second).astype(bf16), earlier_rows.astype(bf16), preferred_element_type=f32
    )
    slot_of = [
        routes[:, k] * capacity + jnp.sum(hit * ahead, axis=0).astype(jnp.int32)
        for k, hit in enumerate((first, second))
    ]
    slots = jnp.arange(expert_total * capacity, dtype=jnp.int32)[:, None]
    named = [(slots == target[None, :]) for target in slot_of]
    pick = (named[0] | named[1]).astype(bf16)
    kind = lax.axis_index("tp") % 2
    scale = [jnp.where(kind == 1, route_weights[:, k], 1.0) for k in range(2)]
    weighted = jnp.where(named[0], scale[0], jnp.where(named[1], scale[1], 0.0)).astype(bf16)
    packed = jnp.dot(
        weighted, jnp.where(kind == 1, cotangent, normed), preferred_element_type=f32
    ).astype(bf16)
    both = dispatch(packed.reshape(groups, slot_span, model_width))
    entry_rows = both[0].reshape(groups * capacity, model_width)
    entry_cots = both[1].reshape(groups * capacity, model_width)
    grads_gate, grads_up, grads_down, terms = ([], [], [], [])
    grad_gate, grad_up, grad_down, partial_sum = expert_pass(
        entry_rows, entry_cots, gate_weight[0], up_weight[0], down_weight[0]
    )
    grads_gate.append(grad_gate)
    grads_up.append(grad_up)
    grads_down.append(grad_down)
    terms.append(partial_sum.astype(bf16).reshape(groups, capacity, model_width))
    expert_term = terms[0]
    summed = (
        lax.psum_scatter(expert_term, "tp", scatter_dimension=2, tiled=True)
        .astype(jnp.float32)
        .astype(bf16)
    )
    returned = lax.all_to_all(summed, "sp", split_axis=0, concat_axis=0, tiled=True).reshape(
        expert_total * capacity, model_width // lanes
    )
    slot_sum = jnp.einsum("jt,jd->td", pick, returned, preferred_element_type=f32)
    dnormed = lax.all_gather(
        slot_sum.astype(jnp.bfloat16), "tp", axis=1, tiled=True
    ).astype(jnp.float32)
    scaled = dnormed * norm_gain
    resid_grad = (
        cotangent.astype(f32)
        + inv_rms * scaled
        - resid_wide * inv_rms**3 * jnp.mean(scaled * resid_wide, axis=1, keepdims=True)
    )
    grad_resid = resid_grad.astype(bf16)
    extended = jnp.concatenate([earlier, mixed], axis=0)
    conv = (
        taps[0] * extended[:token_count]
        + taps[1] * extended[1 : token_count + 1]
        + taps[2] * extended[2 : token_count + 2]
    )
    merged = (gate_b.astype(f32) * conv).astype(bf16)
    grad_out_weight = sum_at_owner(
        jnp.einsum("td,tc->dc", grad_resid, merged, preferred_element_type=f32).astype(
            jnp.bfloat16
        ),
        "sp",
        0,
    )
    dmerged = jnp.dot(grad_resid, out_weight, preferred_element_type=f32)
    grad_gate_b = (dmerged * conv).astype(bf16)
    dconv = dmerged * gate_b.astype(f32)
    later = passed_along(dconv[:2], "sp", -1)
    extended_grad = jnp.concatenate([dconv, later], axis=0)
    dmixed = (
        taps[2] * extended_grad[:token_count]
        + taps[1] * extended_grad[1 : token_count + 1]
        + taps[0] * extended_grad[2 : token_count + 2]
    )
    grad_gate_c = (dmixed * values_u.astype(f32)).astype(bf16)
    grad_values = (dmixed * gate_c.astype(f32)).astype(bf16)
    return (
        jnp.stack(grads_gate),
        jnp.stack(grads_up),
        jnp.stack(grads_down),
        grad_resid,
        grad_out_weight,
        grad_gate_b,
        grad_gate_c,
        grad_values,
    )


def solution(mesh):
    placed = (
        P("sp", None),
        P("sp", None),
        P(),
        P("sp", None),
        P("sp", None),
        P("sp", None, "tp"),
        P("sp", None, "tp"),
        P("sp", "tp", None),
        P(None, "tp"),
        P("sp", "tp"),
        P("sp", "tp"),
        P("sp", "tp"),
        P(None, "tp"),
    )
    return jax.shard_map(
        on_device,
        mesh=mesh,
        in_specs=placed,
        out_specs=(
            P("sp", None, "tp"),
            P("sp", None, "tp"),
            P("sp", "tp", None),
            P("sp", None),
            P("sp", "tp"),
            P("sp", "tp"),
            P("sp", "tp"),
            P("sp", "tp"),
        ),
        check_vma=False,
    )
```

```python
import jax
import jax.numpy as jnp
from jax import lax
from jax.experimental import pallas as pl
from jax.experimental.pallas import tpu as pltpu
from jax.sharding import PartitionSpec as P

norm_eps = 1e-06


def passed_along(array, axis, by):
    size = lax.axis_size(axis)
    pairs = [(i, i + by) for i in range(size) if 0 <= i + by < size]
    return lax.ppermute(array, axis, pairs)


def cut_along(array, dim, size):
    before, after = (array.shape[:dim], array.shape[dim + 1 :])
    return jnp.moveaxis(array.reshape(*before, size, -1, *after), dim, 0)


def sum_at_owner(array, axis, dim):
    size = lax.axis_size(axis)
    tiles = lax.all_to_all(cut_along(array, dim, size), axis, 0, 0, tiled=True)
    return jnp.sum(tiles.astype(jnp.float32), axis=0)


MESH = pl.DeviceIdType.MESH
BF16 = jnp.bfloat16
F32 = jnp.float32
SLOTS = 48
PER_GROUP = 4
GROUP_ROWS = PER_GROUP * SLOTS
GROUPS = 32 // PER_GROUP


def offsets(k):
    m = 7 * k
    return (m // 8) % 4, (m // 2) % 4, m % 2


def moved(s, k, sign):
    z, y, c = s // 8, (s // 2) % 4, s % 2
    dz, dy, dc = offsets(k)
    z = lax.rem(z + 4 + sign * dz, 4)
    y = lax.rem(y + 4 + sign * dy, 4)
    return (z * 4 + y) * 2 + lax.rem(c + dc, 2)


def turn_of(expert, s):
    dz = (expert // 8 - s // 8) % 4
    dy = ((expert // 2) % 4 - (s // 2) % 4) % 4
    dc = (expert - s) % 2
    return (23 * (dz * 8 + dy * 2 + dc)) % 32


def dot_nn(a, b):
    return jnp.dot(a, b, preferred_element_type=F32)


def dot_nt(a, b):
    return lax.dot_general(a, b, (((1,), (1,)), ((), ())), preferred_element_type=F32)


def dot_tn(a, b):
    return lax.dot_general(a, b, (((0,), (0,)), ((), ())), preferred_element_type=F32)


def block(k):
    return pl.ds(pl.multiple_of(k * SLOTS, SLOTS), SLOTS)


def group(g):
    return pl.ds(pl.multiple_of(g * GROUP_ROWS, GROUP_ROWS), GROUP_ROWS)


def wide(j, size):
    return pl.ds(pl.multiple_of(j * size, size), size)


def experts_kernel(
    packed, gate_w, up_w, down_w, pick,
    grad_gate, grad_up, grad_down, total,
    both, part, swapped, summed, back, hidden, dgate, dup, half_out, half_in, half_own,
    far_send, far_recv, near_send, near_recv, swap_send, swap_recv,
    back_send, back_recv, half_send, half_recv, all_send, all_recv, own_sem,
):
    s, x = lax.axis_index("sp"), lax.axis_index("tp")
    kind = lax.rem(x, 2)
    high = x // 2
    right, left, across = lax.rem(x + 1, 4), lax.rem(x + 3, 4), lax.rem(x + 2, 4)
    sides = (right, left)
    given = (1 + 2 * kind, 2 - 2 * kind)
    kept = (2 * kind, 3 - 2 * kind)
    barrier = pltpu.get_barrier_semaphore()

    def greet(k, carry):
        pl.semaphore_signal(
            barrier, inc=1, device_id={"sp": moved(s, k, 1), "tp": x}, device_id_type=MESH
        )
        return carry

    lax.fori_loop(1, 32, greet, 0)
    for lane in (right, left, across):
        pl.semaphore_signal(barrier, inc=1, device_id={"sp": s, "tp": lane}, device_id_type=MESH)
    pl.semaphore_wait(barrier, 34)

    def far(k):
        return pltpu.make_async_remote_copy(
            src_ref=packed.at[block(k)],
            dst_ref=both.at[kind, block(k)],
            send_sem=far_send.at[k],
            recv_sem=far_recv.at[k],
            device_id={"sp": moved(s, k, 1), "tp": x},
            device_id_type=MESH,
        )

    def near(h, k, own=False):
        cols = pl.ds(h * 1024, 1024)
        return pltpu.make_async_remote_copy(
            src_ref=packed.at[block(0), cols] if own else both.at[kind, block(k), cols],
            dst_ref=both.at[kind, block(k), cols],
            send_sem=near_send.at[h, k],
            recv_sem=near_recv.at[h, k],
            device_id={"sp": s, "tp": sides[h]},
            device_id_type=MESH,
        )

    def swap(h, k):
        return pltpu.make_async_remote_copy(
            src_ref=part.at[block(k), wide(given[h], 512)],
            dst_ref=swapped.at[1 - h, block(k)],
            send_sem=swap_send.at[h, k],
            recv_sem=swap_recv.at[h, k],
            device_id={"sp": s, "tp": sides[h]},
            device_id_type=MESH,
        )

    def home(k):
        return pltpu.make_async_remote_copy(
            src_ref=summed.at[block(k)],
            dst_ref=back.at[block(k)],
            send_sem=back_send.at[k],
            recv_sem=back_recv.at[k],
            device_id={"sp": moved(s, k, -1), "tp": x},
            device_id_type=MESH,
        )

    def each(first, last, action):
        def body(k, carry):
            action(k)
            return carry

        lax.fori_loop(first, last, body, 0)

    keep = pltpu.make_async_copy(packed.at[block(0)], both.at[kind, block(0)], own_sem)
    each(1, 32, lambda k: far(k).start())
    keep.start()
    for h in range(2):
        near(h, 0, True).start()
    grad_gate[...] = jnp.zeros_like(grad_gate)
    grad_up[...] = jnp.zeros_like(grad_up)
    grad_down[...] = jnp.zeros_like(grad_down)
    keep.wait()

    def pass_on(k):
        far(k).wait_recv()
        for h in range(2):
            near(h, k).start()

    def arrived(k):
        for h in range(2):
            near(h, k).wait_recv()

    def expert(g):
        rows = group(g)
        row, cot = both[0, rows, :], both[1, rows, :]
        gate = dot_nn(row, gate_w[...])
        up = dot_nn(row, up_w[...])
        dhidden = dot_nt(cot, down_w[...])
        logistic = jax.nn.sigmoid(gate)
        activated = gate * logistic
        hidden[...] = (activated * up).astype(BF16)
        dgate[...] = (dhidden * up * logistic * (1.0 + gate * (1.0 - logistic))).astype(BF16)
        dup[...] = (dhidden * activated).astype(BF16)

        def tile(j):
            cols = wide(j, 512)
            part[rows, cols] = (
                dot_nt(dgate[...], gate_w[cols, :]) + dot_nt(dup[...], up_w[cols, :])
            ).astype(BF16)

        each(0, 4, tile)

    def weights(g):
        rows = group(g)

        def tile(j):
            cols = wide(j, 512)
            row = both[0, rows, cols]
            grad_gate[cols, :] += dot_tn(row, dgate[...])
            grad_up[cols, :] += dot_tn(row, dup[...])
            grad_down[:, cols] += dot_tn(hidden[...], both[1, rows, cols])

        each(0, 4, tile)

    def swap_arrived(k):
        for h in range(2):
            swap(h, k).wait_recv()

    def pair_sum(g):
        rows = group(g)
        for h in range(2):
            summed[rows, pl.ds(h * 512, 512)] = (
                part[rows, wide(kept[h], 512)].astype(F32) + swapped[h, rows, :].astype(F32)
            ).astype(BF16)

    def step(g, carry):
        first = g * PER_GROUP

        @pl.when(g < GROUPS)
        def _():
            each(jnp.maximum(first, 1), first + PER_GROUP, pass_on)

        @pl.when((g >= 1) & (g <= GROUPS))
        def _():
            each(first - PER_GROUP, first, arrived)
            expert(g - 1)

        @pl.when((g >= 2) & (g <= GROUPS + 1))
        def _():
            each(first - 2 * PER_GROUP, first - PER_GROUP, swap_arrived)
            pair_sum(g - 2)

        @pl.when((g >= 1) & (g <= GROUPS))
        def _():
            def send(k):
                for h in range(2):
                    swap(h, k).start()

            each(first - PER_GROUP, first, send)
            weights(g - 1)

        @pl.when((g >= 2) & (g <= GROUPS + 1))
        def _():
            each(jnp.maximum(first - 2 * PER_GROUP, 1), first - PER_GROUP, lambda k: home(k).start())

        return carry

    lax.fori_loop(0, GROUPS + 2, step, 0)
    back[block(0), :] = summed[block(0), :]
    each(1, 32, lambda k: home(k).wait_recv())

    def gathered(half, j):
        return dot_nn(pick[...], back[:, wide(half * 2 + j, 256)])

    for j in range(2):
        half_out[:, pl.ds(j * 256, 256)] = gathered(1 - high, j).astype(BF16)
    cross = pltpu.make_async_remote_copy(
        src_ref=half_out,
        dst_ref=half_in,
        send_sem=half_send,
        recv_sem=half_recv,
        device_id={"sp": s, "tp": across},
        device_id_type=MESH,
    )
    cross.start()
    for j in range(2):
        half_own[:, pl.ds(j * 256, 256)] = gathered(high, j)
    cross.wait()

    def quarter_of(lane):
        odd, upper = lax.rem(lane, 2), lane // 2
        return (1 - upper) * 2 * odd + upper * (3 - 2 * odd)

    total[:, wide(quarter_of(x), 512)] = (half_own[...] + half_in[...].astype(F32)).astype(BF16)
    rows_half = total.shape[0] // 2

    def share(n, owner, h, lane):
        piece = total.at[pl.ds(h * rows_half, rows_half), wide(quarter_of(owner), 512)]
        return pltpu.make_async_remote_copy(
            src_ref=piece,
            dst_ref=piece,
            send_sem=all_send.at[n],
            recv_sem=all_recv.at[n],
            device_id={"sp": s, "tp": lane},
            device_id_type=MESH,
        )

    shares = [
        share(0, x, 0, right),
        share(1, x, 1, right),
        share(2, x, 0, left),
        share(3, x, 1, left),
        share(4, left, 0, right),
        share(5, right, 1, left),
    ]
    for n in (0, 3, 1, 2):
        shares[n].start()
    shares[0].wait_recv()
    shares[4].start()
    shares[3].wait_recv()
    shares[5].start()
    for n in (1, 2, 4, 5):
        shares[n].wait_recv()
    for copy in shares:
        copy.wait_send()

    def finish(k):
        far(k).wait_send()
        home(k).wait_send()
        for h in range(2):
            near(h, k).wait_send()

    each(1, 32, finish)
    for h in range(2):
        near(h, 0, True).wait_send()

    def finish_swap(k):
        for h in range(2):
            swap(h, k).wait_send()

    each(0, 32, finish_swap)


def experts(packed, gate_w, up_w, down_w, pick, token_count):
    vmem = pl.BlockSpec(memory_space=pltpu.VMEM)
    slots, width = packed.shape
    hidden = gate_w.shape[1]
    return pl.pallas_call(
        experts_kernel,
        out_shape=[
            jax.ShapeDtypeStruct((width, hidden), F32),
            jax.ShapeDtypeStruct((width, hidden), F32),
            jax.ShapeDtypeStruct((hidden, width), F32),
            jax.ShapeDtypeStruct((token_count, width), BF16),
        ],
        in_specs=[pl.BlockSpec(memory_space=pl.ANY)] + [vmem] * 4,
        out_specs=[vmem] * 4,
        scratch_shapes=[
            pltpu.VMEM((2, slots, width), BF16),
            pltpu.VMEM((slots, width), BF16),
            pltpu.VMEM((2, slots, 512), BF16),
            pltpu.VMEM((slots, 1024), BF16),
            pltpu.VMEM((slots, 1024), BF16),
            pltpu.VMEM((GROUP_ROWS, hidden), BF16),
            pltpu.VMEM((GROUP_ROWS, hidden), BF16),
            pltpu.VMEM((GROUP_ROWS, hidden), BF16),
            pltpu.VMEM((token_count, 512), BF16),
            pltpu.VMEM((token_count, 512), BF16),
            pltpu.VMEM((token_count, 512), F32),
            pltpu.SemaphoreType.DMA((32,)),
            pltpu.SemaphoreType.DMA((32,)),
            pltpu.SemaphoreType.DMA((2, 32)),
            pltpu.SemaphoreType.DMA((2, 32)),
            pltpu.SemaphoreType.DMA((2, 32)),
            pltpu.SemaphoreType.DMA((2, 32)),
            pltpu.SemaphoreType.DMA((32,)),
            pltpu.SemaphoreType.DMA((32,)),
            pltpu.SemaphoreType.DMA,
            pltpu.SemaphoreType.DMA,
            pltpu.SemaphoreType.DMA((6,)),
            pltpu.SemaphoreType.DMA((6,)),
            pltpu.SemaphoreType.DMA,
        ],
        compiler_params=pltpu.CompilerParams(
            collective_id=0, has_side_effects=True, vmem_limit_bytes=58 * 2**20
        ),
    )(packed, gate_w, up_w, down_w, pick)


def on_device(
    resid_in,
    cotangent,
    norm_gain,
    routes,
    route_weights,
    gate_weight,
    up_weight,
    down_weight,
    out_weight,
    gate_b,
    gate_c,
    values_u,
    taps,
):
    f32 = jnp.float32
    bf16 = jnp.bfloat16
    token_count = resid_in.shape[0]
    groups = lax.axis_size("sp")
    expert_total = groups
    resid_wide = resid_in.astype(f32)
    inv_rms = lax.rsqrt(jnp.mean(resid_wide * resid_wide, axis=1, keepdims=True) + norm_eps)
    normed = (resid_wide * inv_rms * norm_gain).astype(bf16)
    mixed = gate_c.astype(f32) * values_u.astype(f32)
    earlier = passed_along(mixed[-2:], "sp", 1)
    names = jnp.arange(expert_total, dtype=jnp.int32)[:, None]
    first, second = (routes[:, 0] == names).astype(f32), (routes[:, 1] == names).astype(f32)
    order = jnp.arange(token_count)
    ahead = jnp.dot(
        (first + second).astype(bf16),
        (order[:, None] < order[None, :]).astype(bf16),
        preferred_element_type=f32,
    )
    s, kind = lax.axis_index("sp"), lax.axis_index("tp") % 2
    slot_of = [
        turn_of(routes[:, k], s) * SLOTS + jnp.sum(hit * ahead, axis=0).astype(jnp.int32)
        for k, hit in enumerate((first, second))
    ]
    slots = jnp.arange(expert_total * SLOTS, dtype=jnp.int32)
    named = [slots[:, None] == target[None, :] for target in slot_of]
    scale = [jnp.where(kind == 1, route_weights[:, k], 1.0) for k in range(2)]
    weighted = jnp.where(named[0], scale[0], jnp.where(named[1], scale[1], 0.0)).astype(bf16)
    packed = jnp.dot(
        weighted, jnp.where(kind == 1, cotangent, normed), preferred_element_type=f32
    ).astype(bf16)
    pick = (
        (slots[None, :] == slot_of[0][:, None]) | (slots[None, :] == slot_of[1][:, None])
    ).astype(bf16)
    grad_gate, grad_up, grad_down, dnormed = experts(
        packed, gate_weight[0], up_weight[0], down_weight[0], pick, token_count
    )
    dnormed = dnormed.astype(f32)
    scaled = dnormed * norm_gain
    resid_grad = (
        cotangent.astype(f32)
        + inv_rms * scaled
        - resid_wide * inv_rms**3 * jnp.mean(scaled * resid_wide, axis=1, keepdims=True)
    )
    grad_resid = resid_grad.astype(bf16)
    extended = jnp.concatenate([earlier, mixed], axis=0)
    conv = (
        taps[0] * extended[:token_count]
        + taps[1] * extended[1 : token_count + 1]
        + taps[2] * extended[2 : token_count + 2]
    )
    merged = (gate_b.astype(f32) * conv).astype(bf16)
    grad_out_weight = sum_at_owner(
        jnp.einsum("td,tc->dc", grad_resid, merged, preferred_element_type=f32).astype(
            jnp.bfloat16
        ),
        "sp",
        0,
    )
    dmerged = jnp.dot(grad_resid, out_weight, preferred_element_type=f32)
    grad_gate_b = (dmerged * conv).astype(bf16)
    dconv = dmerged * gate_b.astype(f32)
    later = passed_along(dconv[:2], "sp", -1)
    extended_grad = jnp.concatenate([dconv, later], axis=0)
    dmixed = (
        taps[2] * extended_grad[:token_count]
        + taps[1] * extended_grad[1 : token_count + 1]
        + taps[0] * extended_grad[2 : token_count + 2]
    )
    grad_gate_c = (dmixed * values_u.astype(f32)).astype(bf16)
    grad_values = (dmixed * gate_c.astype(f32)).astype(bf16)
    return (
        grad_gate[None],
        grad_up[None],
        grad_down[None],
        grad_resid,
        grad_out_weight,
        grad_gate_b,
        grad_gate_c,
        grad_values,
    )


def solution(mesh):
    placed = (
        P("sp", None),
        P("sp", None),
        P(),
        P("sp", None),
        P("sp", None),
        P("sp", None, "tp"),
        P("sp", None, "tp"),
        P("sp", "tp", None),
        P(None, "tp"),
        P("sp", "tp"),
        P("sp", "tp"),
        P("sp", "tp"),
        P(None, "tp"),
    )
    return jax.shard_map(
        on_device,
        mesh=mesh,
        in_specs=placed,
        out_specs=(
            P("sp", None, "tp"),
            P("sp", None, "tp"),
            P("sp", "tp", None),
            P("sp", None),
            P("sp", "tp"),
            P("sp", "tp"),
            P("sp", "tp"),
            P("sp", "tp"),
        ),
        check_vma=False,
    )
```

```python
import jax
import jax.numpy as jnp
from jax import lax
from jax.experimental import pallas as pl
from jax.experimental.pallas import tpu as pltpu
from jax.sharding import PartitionSpec as P

norm_eps = 1e-06


MESH = pl.DeviceIdType.MESH
BF16 = jnp.bfloat16
F32 = jnp.float32
SLOTS = 48
PER_GROUP = 2
GROUP_ROWS = PER_GROUP * SLOTS
GROUPS = 32 // PER_GROUP


def offsets(k):
    m = 7 * k
    return (m // 8) % 4, (m // 2) % 4, m % 2


def moved(s, k, sign):
    z, y, c = s // 8, (s // 2) % 4, s % 2
    dz, dy, dc = offsets(k)
    z = lax.rem(z + 4 + sign * dz, 4)
    y = lax.rem(y + 4 + sign * dy, 4)
    return (z * 4 + y) * 2 + lax.rem(c + dc, 2)


def turn_of(expert, s):
    dz = (expert // 8 - s // 8) % 4
    dy = ((expert // 2) % 4 - (s // 2) % 4) % 4
    dc = (expert - s) % 2
    return (23 * (dz * 8 + dy * 2 + dc)) % 32


def dot_nn(a, b):
    return jnp.dot(a, b, preferred_element_type=F32)


def dot_nt(a, b):
    return lax.dot_general(a, b, (((1,), (1,)), ((), ())), preferred_element_type=F32)


def dot_tn(a, b):
    return lax.dot_general(a, b, (((0,), (0,)), ((), ())), preferred_element_type=F32)


def block(k):
    return pl.ds(pl.multiple_of(k * SLOTS, SLOTS), SLOTS)


def group(g):
    return pl.ds(pl.multiple_of(g * GROUP_ROWS, GROUP_ROWS), GROUP_ROWS)


def wide(j, size):
    return pl.ds(pl.multiple_of(j * size, size), size)


PARTNER = 23
EARLY = 5
EDGE = 8


def experts_kernel(
    resid, cots, gain, slot, weight, slot_col, gate_w, up_w, down_w, out_w,
    gate_b, gate_c, values, taps,
    grad_gate, grad_up, grad_down, grad_resid, grad_out, grad_b, grad_c, grad_values,
    both, part, extra, swapped, back, hidden, dgate, dup, half_out, half_in, half_own,
    normed, inverse, pick, total, mixed, conv, merged, dconv, staged, gathered,
    far_send, far_recv, near_send, near_recv, swap_send, swap_recv, back_send, back_recv,
    out_send, out_recv, all_send, all_recv,
    extra_send, extra_recv, half_send, half_recv, later_send, later_recv, sooner_send, sooner_recv,
):
    s, x = lax.axis_index("sp"), lax.axis_index("tp")
    kind = lax.rem(x, 2)
    high = x // 2
    right, left, across = lax.rem(x + 1, 4), lax.rem(x + 3, 4), lax.rem(x + 2, 4)
    sides = (right, left)
    given = (1 + 2 * kind, 2 - 2 * kind)
    kept = (2 * kind, 3 - 2 * kind)
    tokens = cots.shape[0]
    barrier = pltpu.get_barrier_semaphore()

    def each(first, last, action):
        def body(k, carry):
            action(k)
            return carry

        lax.fori_loop(first, last, body, 0)

    def greet(k):
        pl.semaphore_signal(
            barrier, inc=1, device_id={"sp": moved(s, k, 1), "tp": x}, device_id_type=MESH
        )

    each(1, 32, greet)
    for lane in (right, left, across):
        pl.semaphore_signal(barrier, inc=1, device_id={"sp": s, "tp": lane}, device_id_type=MESH)

    def remote(source, target, sent, received, sp, tp):
        return pltpu.make_async_remote_copy(
            src_ref=source,
            dst_ref=target,
            send_sem=sent,
            recv_sem=received,
            device_id={"sp": sp, "tp": tp},
            device_id_type=MESH,
        )

    def far(k):
        return remote(
            part.at[block(k)], both.at[kind, block(k)], far_send.at[k], far_recv.at[k],
            moved(s, k, 1), x,
        )

    def near(h, k):
        piece = both.at[kind, block(k), pl.ds(h * 1024, 1024)]
        return remote(piece, piece, near_send.at[h, k], near_recv.at[h, k], s, sides[h])

    def swap(h, k):
        return remote(
            part.at[block(k), wide(given[h], 512)],
            swapped.at[block(k), pl.ds((1 - h) * 512, 512)],
            swap_send.at[h, k], swap_recv.at[h, k], s, sides[h],
        )

    def home(k):
        return remote(
            swapped.at[block(k)], back.at[block(k)], back_send.at[k], back_recv.at[k],
            moved(s, k, -1), x,
        )

    other = remote(
        extra, both.at[1 - kind, block(PARTNER)], extra_send, extra_recv, moved(s, PARTNER, 1), x
    )
    later = remote(
        mixed.at[pl.ds(tokens, EDGE)], mixed.at[pl.ds(0, EDGE)], later_send, later_recv,
        jnp.minimum(s + 1, 31), x,
    )
    sooner = remote(
        dconv.at[pl.ds(0, EDGE)], dconv.at[pl.ds(tokens, EDGE)], sooner_send, sooner_recv,
        jnp.maximum(s - 1, 0), x,
    )

    def normalize(i):
        rows = wide(i, 64)
        held = resid[rows, :].astype(F32)
        scale = lax.rsqrt(jnp.mean(held * held, axis=1, keepdims=True) + norm_eps)
        normed[rows, :] = (held * scale * gain[...]).astype(BF16)
        inverse[rows, :] = jnp.broadcast_to(scale, (64, 128))

    each(0, tokens // 64, normalize)

    def pack(target, rows, first, count, is_cot):
        ids = lax.broadcasted_iota(jnp.int32, (count * SLOTS, tokens), 0) + first * SLOTS
        zero = jnp.zeros((count * SLOTS, tokens), F32)
        ones = jnp.ones((1, tokens), F32)
        value = [weight[k : k + 1, :] if is_cot else ones for k in range(2)]
        chosen = jnp.where(
            ids == slot[0:1, :], value[0], jnp.where(ids == slot[1:2, :], value[1], zero)
        ).astype(BF16)
        data = cots if is_cot else normed
        for j in range(4):
            cols = pl.ds(j * 512, 512)
            target[rows, cols] = dot_nn(chosen, data[:, cols]).astype(BF16)

    def pack_group(g):
        for option in range(2):

            @pl.when(kind == option)
            def _():
                rows = wide(g, 4 * SLOTS)
                pack(part, rows, g * 4, 4, option == 1)

    pack_group(0)
    mixed[pl.ds(EDGE, tokens), :] = gate_c[...].astype(F32) * values[...].astype(F32)
    pl.semaphore_wait(barrier, 34)

    def pass_on(k):
        far(k).wait_recv()

        @pl.when(k != PARTNER)
        def _():
            for h in range(2):
                near(h, k).start()

    def pack_and_send(g, carry):
        pack_group(g)
        each(jnp.maximum(g * 4 - 4, 1), g * 4, lambda k: far(k).start())

        @pl.when(g >= 4)
        def _():
            pass_on(g - 3)

        return carry

    lax.fori_loop(1, 8, pack_and_send, 0)
    each(28, 32, lambda k: far(k).start())

    @pl.when(s < 31)
    def _():
        later.start()

    for option in range(2):
        pack(both.at[option], pl.ds(0, SLOTS), 0, 1, option == 1)

        @pl.when(kind == option)
        def _():
            pack(extra, pl.ds(0, SLOTS), PARTNER, 1, option == 0)

    def arrived(k):
        @pl.when((k != PARTNER) & (k != 0))
        def _():
            for h in range(2):
                near(h, k).wait_recv()

        @pl.when(k == PARTNER)
        def _():
            other.wait_recv()

    def expert(g):
        rows = group(g)
        local = wide(lax.rem(g, 2), GROUP_ROWS)
        row, cot = both[0, rows, :], both[1, rows, :]
        gate = dot_nn(row, gate_w[...])
        up = dot_nn(row, up_w[...])
        dhidden = dot_nt(cot, down_w[...])
        logistic = jax.nn.sigmoid(gate)
        activated = gate * logistic
        hidden[local, :] = (activated * up).astype(BF16)
        dgate[local, :] = (dhidden * up * logistic * (1.0 + gate * (1.0 - logistic))).astype(BF16)
        dup[local, :] = (dhidden * activated).astype(BF16)

        def tile(j):
            cols = wide(j, 512)
            part[rows, cols] = (
                dot_nt(dgate[local, :], gate_w[cols, :]) + dot_nt(dup[local, :], up_w[cols, :])
            ).astype(BF16)

        each(0, 4, tile)

    def weights(chunk):
        rows = wide(chunk, 2 * GROUP_ROWS)

        def tile(j):
            cols = wide(j, 512)
            row = both[0, rows, cols]
            grad_gate[cols, :] += dot_tn(row, dgate[...])
            grad_up[cols, :] += dot_tn(row, dup[...])
            grad_down[:, cols] += dot_tn(hidden[...], both[1, rows, cols])

        each(0, 4, tile)

    def swap_arrived(k):
        for h in range(2):
            swap(h, k).wait_recv()

    def pair_sum(g):
        rows = group(g)
        for h in range(2):
            cols = pl.ds(h * 512, 512)
            swapped[rows, cols] = (
                part[rows, wide(kept[h], 512)].astype(F32) + swapped[rows, cols].astype(F32)
            ).astype(BF16)

    def make_pick():
        ids = lax.broadcasted_iota(jnp.int32, pick.shape, 1)
        hit = (ids == slot_col[:, 0:1]) | (ids == slot_col[:, 1:2])
        pick[...] = jnp.where(hit, 1.0, 0.0).astype(BF16)

    def make_conv():
        @pl.when(s == 0)
        def _():
            mixed[pl.ds(0, EDGE), :] = jnp.zeros((EDGE, mixed.shape[1]), F32)

        @pl.when(s > 0)
        def _():
            later.wait_recv()

        conv[...] = (
            taps[0:1, :] * mixed[pl.ds(EDGE - 2, tokens), :]
            + taps[1:2, :] * mixed[pl.ds(EDGE - 1, tokens), :]
            + taps[2:3, :] * mixed[pl.ds(EDGE, tokens), :]
        )
        merged[...] = (gate_b[...].astype(F32) * conv[...]).astype(BF16)

    def step(g, carry):
        first = g * PER_GROUP

        @pl.when(g < GROUPS)
        def _():
            each(jnp.maximum(first, EARLY), first + PER_GROUP, pass_on)

        @pl.when(g == 0)
        def _():
            other.start()
            grad_gate[...] = jnp.zeros_like(grad_gate)
            grad_up[...] = jnp.zeros_like(grad_up)
            grad_down[...] = jnp.zeros_like(grad_down)

        @pl.when((g >= 1) & (g <= GROUPS))
        def _():
            each(first - PER_GROUP, first, arrived)
            each(jnp.maximum(first - PER_GROUP, 1), first, lambda k: far(k).wait_send())
            expert(g - 1)

        @pl.when((g >= 2) & (g <= GROUPS + 1))
        def _():
            each(first - 2 * PER_GROUP, first - PER_GROUP, swap_arrived)
            pair_sum(g - 2)

        @pl.when((g >= 1) & (g <= GROUPS))
        def _():
            def send(k):
                for h in range(2):
                    swap(h, k).start()

            each(first - PER_GROUP, first, send)

        @pl.when((g >= 2) & (g < GROUPS) & (lax.rem(g, 2) == 0))
        def _():
            weights(g // 2 - 1)

        @pl.when(g == 3)
        def _():
            make_pick()

        @pl.when(g == 5)
        def _():
            make_conv()

        @pl.when((g >= 2) & (g <= GROUPS + 1))
        def _():
            each(jnp.maximum(first - 2 * PER_GROUP, 1), first - PER_GROUP, lambda k: home(k).start())

        return carry

    lax.fori_loop(0, GROUPS + 2, step, 0)
    back[block(0), :] = swapped[block(0), :]
    weights(GROUPS // 2 - 1)
    each(1, 32, lambda k: home(k).wait_recv())

    def summed(half, j):
        return dot_nn(pick[...], back[:, wide(half * 2 + j, 256)])

    for j in range(2):
        half_out[:, pl.ds(j * 256, 256)] = summed(1 - high, j).astype(BF16)
    cross = remote(half_out, half_in, half_send, half_recv, s, across)
    cross.start()
    for j in range(2):
        half_own[:, pl.ds(j * 256, 256)] = summed(high, j)
    cross.wait()

    def quarter_of(lane):
        odd, upper = lax.rem(lane, 2), lane // 2
        return (1 - upper) * 2 * odd + upper * (3 - 2 * odd)

    total[:, wide(quarter_of(x), 512)] = (half_own[...] + half_in[...].astype(F32)).astype(BF16)

    def share(n, owner, h, lane):
        piece = total.at[pl.ds(h * (tokens // 2), tokens // 2), wide(quarter_of(owner), 512)]
        return remote(piece, piece, all_send.at[n], all_recv.at[n], s, lane)

    shares = [
        share(0, x, 0, right),
        share(1, x, 1, right),
        share(2, x, 0, left),
        share(3, x, 1, left),
        share(4, left, 0, right),
        share(5, right, 1, left),
    ]
    for n in (0, 3, 1, 2):
        shares[n].start()
    shares[0].wait_recv()
    shares[4].start()
    shares[3].wait_recv()
    shares[5].start()
    for n in (1, 2, 4, 5):
        shares[n].wait_recv()
    for copy in shares:
        copy.wait_send()

    def resid_tile(i):
        rows = wide(i, 64)
        scaled = total[rows, :].astype(F32) * gain[...]
        held = resid[rows, :].astype(F32)
        scale = inverse[rows, 0:1]
        mean = jnp.mean(scaled * held, axis=1, keepdims=True)
        grad_resid[rows, :] = (
            cots[rows, :].astype(F32) + scale * scaled - held * (scale * scale * scale * mean)
        ).astype(BF16)

    each(0, tokens // 64, resid_tile)
    for j in range(4):
        cols = pl.ds(j * 512, 512)
        staged[cols, :] = dot_tn(grad_resid[:, cols], merged[...]).astype(BF16)
    share_rows = grad_out.shape[0]

    def give(k):
        owner = moved(s, k, 1)
        return remote(
            staged.at[wide(owner, share_rows)], gathered.at[k], out_send.at[k], out_recv.at[k],
            owner, x,
        )

    dmerged = dot_nn(grad_resid[...], out_w[...])
    dconv[pl.ds(0, tokens), :] = dmerged * gate_b[...].astype(F32)
    grad_b[...] = (dmerged * conv[...]).astype(BF16)
    each(1, 32, lambda k: give(k).start())

    @pl.when(s > 0)
    def _():
        sooner.start()

    @pl.when(s == 31)
    def _():
        dconv[pl.ds(tokens, EDGE), :] = jnp.zeros((EDGE, dconv.shape[1]), F32)

    gathered[0] = staged[wide(s, share_rows), :]

    def finish(k):
        home(k).wait_send()

        @pl.when(k != PARTNER)
        def _():
            for h in range(2):
                near(h, k).wait_send()

    each(1, 32, finish)

    def finish_swap(k):
        for h in range(2):
            swap(h, k).wait_send()

    each(0, 32, finish_swap)
    other.wait_send()

    @pl.when(s < 31)
    def _():
        later.wait_send()
        sooner.wait_recv()

    dmixed = (
        taps[2:3, :] * dconv[pl.ds(0, tokens), :]
        + taps[1:2, :] * dconv[pl.ds(1, tokens), :]
        + taps[0:1, :] * dconv[pl.ds(2, tokens), :]
    )
    grad_c[...] = (dmixed * values[...].astype(F32)).astype(BF16)
    grad_values[...] = (dmixed * gate_c[...].astype(F32)).astype(BF16)
    each(1, 32, lambda k: give(k).wait_recv())
    grad_out[...] = jnp.sum(gathered[...].astype(F32), axis=0)
    each(1, 32, lambda k: give(k).wait_send())

    @pl.when(s > 0)
    def _():
        sooner.wait_send()


def on_device(
    resid_in,
    cotangent,
    norm_gain,
    routes,
    route_weights,
    gate_weight,
    up_weight,
    down_weight,
    out_weight,
    gate_b,
    gate_c,
    values_u,
    taps,
):
    tokens, width = resid_in.shape
    hidden, channels = gate_weight.shape[2], gate_b.shape[1]
    experts = lax.axis_size("sp")
    slots = experts * SLOTS
    names = jnp.arange(experts, dtype=jnp.int32)[:, None]
    first, second = (routes[:, 0] == names).astype(F32), (routes[:, 1] == names).astype(F32)
    order = jnp.arange(tokens)
    ahead = jnp.dot(
        (first + second).astype(BF16),
        (order[:, None] < order[None, :]).astype(BF16),
        preferred_element_type=F32,
    )
    s = lax.axis_index("sp")
    slot = jnp.stack(
        [
            turn_of(routes[:, k], s) * SLOTS + jnp.sum(hit * ahead, axis=0).astype(jnp.int32)
            for k, hit in enumerate((first, second))
        ]
    )
    vmem = pl.BlockSpec(memory_space=pltpu.VMEM)
    dma = pltpu.SemaphoreType.DMA
    outs = pl.pallas_call(
        experts_kernel,
        out_shape=[
            jax.ShapeDtypeStruct((width, hidden), F32),
            jax.ShapeDtypeStruct((width, hidden), F32),
            jax.ShapeDtypeStruct((hidden, width), F32),
            jax.ShapeDtypeStruct((tokens, width), BF16),
            jax.ShapeDtypeStruct((width // experts, channels), F32),
            jax.ShapeDtypeStruct((tokens, channels), BF16),
            jax.ShapeDtypeStruct((tokens, channels), BF16),
            jax.ShapeDtypeStruct((tokens, channels), BF16),
        ],
        in_specs=[vmem] * 14,
        out_specs=[vmem] * 8,
        scratch_shapes=[
            pltpu.VMEM((2, slots, width), BF16),
            pltpu.VMEM((slots, width), BF16),
            pltpu.VMEM((SLOTS, width), BF16),
            pltpu.VMEM((slots, 1024), BF16),
            pltpu.VMEM((slots, 1024), BF16),
            pltpu.VMEM((2 * GROUP_ROWS, hidden), BF16),
            pltpu.VMEM((2 * GROUP_ROWS, hidden), BF16),
            pltpu.VMEM((2 * GROUP_ROWS, hidden), BF16),
            pltpu.VMEM((tokens, 512), BF16),
            pltpu.VMEM((tokens, 512), BF16),
            pltpu.VMEM((tokens, 512), F32),
            pltpu.VMEM((tokens, width), BF16),
            pltpu.VMEM((tokens, 128), F32),
            pltpu.VMEM((tokens, slots), BF16),
            pltpu.VMEM((tokens, width), BF16),
            pltpu.VMEM((tokens + EDGE, channels), F32),
            pltpu.VMEM((tokens, channels), F32),
            pltpu.VMEM((tokens, channels), BF16),
            pltpu.VMEM((tokens + EDGE, channels), F32),
            pltpu.VMEM((width, channels), BF16),
            pltpu.VMEM((experts, width // experts, channels), BF16),
        ]
        + [dma((32,)), dma((32,)), dma((2, 32)), dma((2, 32)), dma((2, 32)), dma((2, 32))]
        + [dma((32,))] * 4
        + [dma((6,))] * 2
        + [dma] * 8,
        compiler_params=pltpu.CompilerParams(
            collective_id=0, has_side_effects=True, vmem_limit_bytes=63 * 2**20
        ),
    )(
        resid_in, cotangent, norm_gain[None], slot, route_weights.T, slot.T,
        gate_weight[0], up_weight[0], down_weight[0], out_weight,
        gate_b, gate_c, values_u, taps,
    )
    return (outs[0][None], outs[1][None], outs[2][None], *outs[3:])


def solution(mesh):
    placed = (
        P("sp", None),
        P("sp", None),
        P(),
        P("sp", None),
        P("sp", None),
        P("sp", None, "tp"),
        P("sp", None, "tp"),
        P("sp", "tp", None),
        P(None, "tp"),
        P("sp", "tp"),
        P("sp", "tp"),
        P("sp", "tp"),
        P(None, "tp"),
    )
    return jax.shard_map(
        on_device,
        mesh=mesh,
        in_specs=placed,
        out_specs=(
            P("sp", None, "tp"),
            P("sp", None, "tp"),
            P("sp", "tp", None),
            P("sp", None),
            P("sp", "tp"),
            P("sp", "tp"),
            P("sp", "tp"),
            P("sp", "tp"),
        ),
        check_vma=False,
    )
```

```python
import jax
import jax.numpy as jnp
from jax import lax
from jax.experimental import pallas as pl
from jax.experimental.pallas import tpu as pltpu
from jax.sharding import PartitionSpec as P

norm_eps = 1e-06


MESH = pl.DeviceIdType.MESH
BF16 = jnp.bfloat16
F32 = jnp.float32
SLOTS = 48
PER_GROUP = 4
GROUP_ROWS = PER_GROUP * SLOTS
GROUPS = 32 // PER_GROUP


def offsets(k):
    m = 7 * k
    return (m // 8) % 4, (m // 2) % 4, m % 2


def moved(s, k, sign):
    z, y, c = s // 8, (s // 2) % 4, s % 2
    dz, dy, dc = offsets(k)
    z = lax.rem(z + 4 + sign * dz, 4)
    y = lax.rem(y + 4 + sign * dy, 4)
    return (z * 4 + y) * 2 + lax.rem(c + dc, 2)


def turn_of(expert, s):
    dz = (expert // 8 - s // 8) % 4
    dy = ((expert // 2) % 4 - (s // 2) % 4) % 4
    dc = (expert - s) % 2
    return (23 * (dz * 8 + dy * 2 + dc)) % 32


def dot_nn(a, b):
    return jnp.dot(a, b, preferred_element_type=F32)


def dot_nt(a, b):
    return lax.dot_general(a, b, (((1,), (1,)), ((), ())), preferred_element_type=F32)


def dot_tn(a, b):
    return lax.dot_general(a, b, (((0,), (0,)), ((), ())), preferred_element_type=F32)


def block(k):
    return pl.ds(pl.multiple_of(k * SLOTS, SLOTS), SLOTS)


def group(g):
    return pl.ds(pl.multiple_of(g * GROUP_ROWS, GROUP_ROWS), GROUP_ROWS)


def wide(j, size):
    return pl.ds(pl.multiple_of(j * size, size), size)


PARTNER = 23
EARLY = 5
EDGE = 8


def experts_kernel(
    resid, cots, gain, slot, weight, slot_col, gate_b, gate_c, values, taps,
    gate_far, up_far, down_far, out_far,
    to_gate, to_up, to_down, to_resid, to_out, to_b, to_c, to_values,
    gate_w, up_w, down_w, out_w,
    grad_gate, grad_up, grad_down, grad_resid, grad_out, grad_b, grad_c, grad_values,
    load_sem, store_sem,
    both, part, extra, swapped, back, hidden, dgate, dup, half_out, half_in, half_own,
    normed, inverse, pick, total, mixed, conv, merged, dconv, staged, inbox, gathered,
    far_send, far_recv, near_send, near_recv, swap_send, swap_recv, back_send, back_recv,
    out_send, out_recv, all_send, all_recv,
    extra_send, extra_recv, half_send, half_recv, later_send, later_recv, sooner_send, sooner_recv,
    inbox_send, inbox_recv,
):
    s, x = lax.axis_index("sp"), lax.axis_index("tp")
    kind = lax.rem(x, 2)
    high = x // 2
    right, left, across = lax.rem(x + 1, 4), lax.rem(x + 3, 4), lax.rem(x + 2, 4)
    sides = (right, left)
    given = (1 + 2 * kind, 2 - 2 * kind)
    kept = (2 * kind, 3 - 2 * kind)
    tokens = cots.shape[0]
    barrier = pltpu.get_barrier_semaphore()

    def each(first, last, action):
        def body(k, carry):
            action(k)
            return carry

        lax.fori_loop(first, last, body, 0)

    def greet(k):
        pl.semaphore_signal(
            barrier, inc=1, device_id={"sp": moved(s, k, 1), "tp": x}, device_id_type=MESH
        )

    loads = [
        pltpu.make_async_copy(source, target, load_sem.at[i])
        for i, (source, target) in enumerate(
            ((gate_far, gate_w), (up_far, up_w), (down_far, down_w), (out_far, out_w))
        )
    ]
    stores = [
        pltpu.make_async_copy(source, target, store_sem.at[i])
        for i, (source, target) in enumerate(
            (
                (grad_gate, to_gate), (grad_up, to_up), (grad_down, to_down),
                (grad_resid, to_resid), (grad_out, to_out), (grad_b, to_b),
                (grad_c, to_c), (grad_values, to_values),
            )
        )
    ]
    each(1, 32, greet)
    for lane in (right, left, across):
        pl.semaphore_signal(barrier, inc=1, device_id={"sp": s, "tp": lane}, device_id_type=MESH)

    def remote(source, target, sent, received, sp, tp):
        return pltpu.make_async_remote_copy(
            src_ref=source,
            dst_ref=target,
            send_sem=sent,
            recv_sem=received,
            device_id={"sp": sp, "tp": tp},
            device_id_type=MESH,
        )

    def far(k):
        return remote(
            part.at[block(k)], both.at[kind, block(k)], far_send.at[k], far_recv.at[k],
            moved(s, k, 1), x,
        )

    def near(h, k):
        piece = both.at[kind, block(k), pl.ds(h * 1024, 1024)]
        return remote(piece, piece, near_send.at[h, k], near_recv.at[h, k], s, sides[h])

    def swap(h, k):
        return remote(
            part.at[block(k), wide(given[h], 512)],
            swapped.at[block(k), pl.ds((1 - h) * 512, 512)],
            swap_send.at[h, k], swap_recv.at[h, k], s, sides[h],
        )

    def home(k):
        return remote(
            swapped.at[block(k)], back.at[block(k)], back_send.at[k], back_recv.at[k],
            moved(s, k, -1), x,
        )

    other = remote(
        extra, both.at[1 - kind, block(PARTNER)], extra_send, extra_recv, moved(s, PARTNER, 1), x
    )
    later = remote(
        mixed.at[pl.ds(tokens, EDGE)], mixed.at[pl.ds(0, EDGE)], later_send, later_recv,
        jnp.minimum(s + 1, 31), x,
    )
    sooner = remote(
        dconv.at[pl.ds(0, EDGE)], dconv.at[pl.ds(tokens, EDGE)], sooner_send, sooner_recv,
        jnp.maximum(s - 1, 0), x,
    )

    def normalize(i):
        rows = wide(i, 64)
        held = resid[rows, :].astype(F32)
        scale = lax.rsqrt(jnp.mean(held * held, axis=1, keepdims=True) + norm_eps)
        normed[rows, :] = (held * scale * gain[...]).astype(BF16)
        inverse[rows, :] = jnp.broadcast_to(scale, (64, 128))

    for copy in loads:
        copy.start()
    each(0, tokens // 64, normalize)

    def pack(target, rows, first, count, is_cot):
        ids = lax.broadcasted_iota(jnp.int32, (count * SLOTS, tokens), 0) + first * SLOTS
        zero = jnp.zeros((count * SLOTS, tokens), F32)
        ones = jnp.ones((1, tokens), F32)
        value = [weight[k : k + 1, :] if is_cot else ones for k in range(2)]
        chosen = jnp.where(
            ids == slot[0:1, :], value[0], jnp.where(ids == slot[1:2, :], value[1], zero)
        ).astype(BF16)
        data = cots if is_cot else normed
        for j in range(4):
            cols = pl.ds(j * 512, 512)
            target[rows, cols] = dot_nn(chosen, data[:, cols]).astype(BF16)

    def pack_group(g):
        for option in range(2):

            @pl.when(kind == option)
            def _():
                rows = wide(g, 4 * SLOTS)
                pack(part, rows, g * 4, 4, option == 1)

    pack_group(0)
    mixed[pl.ds(EDGE, tokens), :] = gate_c[...].astype(F32) * values[...].astype(F32)
    pl.semaphore_wait(barrier, 34)

    def pass_on(k):
        far(k).wait_recv()

        @pl.when(k != PARTNER)
        def _():
            for h in range(2):
                near(h, k).start()

    def pack_and_send(g, carry):
        pack_group(g)
        each(jnp.maximum(g * 4 - 4, 1), g * 4, lambda k: far(k).start())

        @pl.when(g >= 4)
        def _():
            pass_on(g - 3)

        return carry

    lax.fori_loop(1, 8, pack_and_send, 0)
    each(28, 32, lambda k: far(k).start())

    @pl.when(s < 31)
    def _():
        later.start()

    for option in range(2):
        pack(both.at[option], pl.ds(0, SLOTS), 0, 1, option == 1)

        @pl.when(kind == option)
        def _():
            pack(extra, pl.ds(0, SLOTS), PARTNER, 1, option == 0)

    def arrived(k):
        @pl.when((k != PARTNER) & (k != 0))
        def _():
            for h in range(2):
                near(h, k).wait_recv()

        @pl.when(k == PARTNER)
        def _():
            other.wait_recv()

    def expert(g):
        rows = group(g)
        local = wide(lax.rem(g, 2), GROUP_ROWS)
        row, cot = both[0, rows, :], both[1, rows, :]
        gate = dot_nn(row, gate_w[...])
        up = dot_nn(row, up_w[...])
        dhidden = dot_nt(cot, down_w[...])
        logistic = jax.nn.sigmoid(gate)
        activated = gate * logistic
        hidden[local, :] = (activated * up).astype(BF16)
        dgate[local, :] = (dhidden * up * logistic * (1.0 + gate * (1.0 - logistic))).astype(BF16)
        dup[local, :] = (dhidden * activated).astype(BF16)

        def tile(j):
            cols = wide(j, 512)
            part[rows, cols] = (
                dot_nt(dgate[local, :], gate_w[cols, :]) + dot_nt(dup[local, :], up_w[cols, :])
            ).astype(BF16)

        each(0, 4, tile)

    def weights(chunk):
        rows = wide(chunk, 2 * GROUP_ROWS)

        def tile(j):
            cols = wide(j, 512)
            row = both[0, rows, cols]
            grad_gate[cols, :] += dot_tn(row, dgate[...])
            grad_up[cols, :] += dot_tn(row, dup[...])
            grad_down[:, cols] += dot_tn(hidden[...], both[1, rows, cols])

        each(0, 4, tile)

    def swap_arrived(k):
        for h in range(2):
            swap(h, k).wait_recv()

    def pair_sum(g):
        rows = group(g)
        for h in range(2):
            cols = pl.ds(h * 512, 512)
            swapped[rows, cols] = (
                part[rows, wide(kept[h], 512)].astype(F32) + swapped[rows, cols].astype(F32)
            ).astype(BF16)

    def make_pick():
        ids = lax.broadcasted_iota(jnp.int32, pick.shape, 1)
        hit = (ids == slot_col[:, 0:1]) | (ids == slot_col[:, 1:2])
        pick[...] = jnp.where(hit, 1.0, 0.0).astype(BF16)

    def make_conv():
        @pl.when(s == 0)
        def _():
            mixed[pl.ds(0, EDGE), :] = jnp.zeros((EDGE, mixed.shape[1]), F32)

        @pl.when(s > 0)
        def _():
            later.wait_recv()

        conv[...] = (
            taps[0:1, :] * mixed[pl.ds(EDGE - 2, tokens), :]
            + taps[1:2, :] * mixed[pl.ds(EDGE - 1, tokens), :]
            + taps[2:3, :] * mixed[pl.ds(EDGE, tokens), :]
        )
        merged[...] = (gate_b[...].astype(F32) * conv[...]).astype(BF16)

    def step(g, carry):
        first = g * PER_GROUP

        @pl.when(g < GROUPS)
        def _():
            each(jnp.maximum(first, EARLY), first + PER_GROUP, pass_on)

        @pl.when(g == 0)
        def _():
            other.start()
            for copy in loads:
                copy.wait()
            grad_gate[...] = jnp.zeros_like(grad_gate)
            grad_up[...] = jnp.zeros_like(grad_up)
            grad_down[...] = jnp.zeros_like(grad_down)

        @pl.when((g >= 1) & (g <= GROUPS))
        def _():
            each(first - PER_GROUP, first, arrived)
            each(jnp.maximum(first - PER_GROUP, 1), first, lambda k: far(k).wait_send())
            expert(g - 1)

        @pl.when((g >= 2) & (g <= GROUPS + 1))
        def _():
            each(first - 2 * PER_GROUP, first - PER_GROUP, swap_arrived)
            pair_sum(g - 2)

        @pl.when((g >= 1) & (g <= GROUPS))
        def _():
            def send(k):
                for h in range(2):
                    swap(h, k).start()

            each(first - PER_GROUP, first, send)

        @pl.when((g >= 2) & (g < GROUPS) & (lax.rem(g, 2) == 0))
        def _():
            weights(g // 2 - 1)

        @pl.when(g == 3)
        def _():
            make_pick()

        @pl.when(g == 5)
        def _():
            make_conv()

        @pl.when((g >= 2) & (g <= GROUPS + 1))
        def _():
            each(jnp.maximum(first - 2 * PER_GROUP, 1), first - PER_GROUP, lambda k: home(k).start())

        return carry

    lax.fori_loop(0, GROUPS + 2, step, 0)
    back[block(0), :] = swapped[block(0), :]
    weights(GROUPS // 2 - 1)
    each(1, 32, lambda k: home(k).wait_recv())
    for copy in stores[:3]:
        copy.start()

    def summed(half, j):
        return dot_nn(pick[...], back[:, wide(half * 2 + j, 256)])

    for j in range(2):
        half_out[:, pl.ds(j * 256, 256)] = summed(1 - high, j).astype(BF16)
    cross = remote(half_out, half_in, half_send, half_recv, s, across)
    cross.start()
    for j in range(2):
        half_own[:, pl.ds(j * 256, 256)] = summed(high, j)
    cross.wait()

    def quarter_of(lane):
        odd, upper = lax.rem(lane, 2), lane // 2
        return (1 - upper) * 2 * odd + upper * (3 - 2 * odd)

    total[:, wide(quarter_of(x), 512)] = (half_own[...] + half_in[...].astype(F32)).astype(BF16)

    def share(n, owner, h, lane):
        piece = total.at[pl.ds(h * (tokens // 2), tokens // 2), wide(quarter_of(owner), 512)]
        return remote(piece, piece, all_send.at[n], all_recv.at[n], s, lane)

    shares = [
        share(0, x, 0, right),
        share(1, x, 1, right),
        share(2, x, 0, left),
        share(3, x, 1, left),
        share(4, left, 0, right),
        share(5, right, 1, left),
    ]
    for n in (0, 3, 1, 2):
        shares[n].start()
    shares[0].wait_recv()
    shares[4].start()
    shares[3].wait_recv()
    shares[5].start()
    for n in (1, 2, 4, 5):
        shares[n].wait_recv()
    for copy in shares:
        copy.wait_send()

    def resid_tile(i):
        rows = wide(i, 64)
        scaled = total[rows, :].astype(F32) * gain[...]
        held = resid[rows, :].astype(F32)
        scale = inverse[rows, 0:1]
        mean = jnp.mean(scaled * held, axis=1, keepdims=True)
        grad_resid[rows, :] = (
            cots[rows, :].astype(F32) + scale * scaled - held * (scale * scale * scale * mean)
        ).astype(BF16)

    each(0, tokens // 64, resid_tile)
    share_rows = grad_out.shape[0]
    core, chip = lax.rem(s, 2), s // 2
    for j in range(4):
        cols = pl.ds(j * 512, 512)
        piece = dot_tn(grad_resid[:, cols], merged[...]).astype(BF16)
        for i in range(8):
            staged[i % 2, pl.ds((j * 4 + i // 2) * share_rows, share_rows), :] = piece[
                i * share_rows : (i + 1) * share_rows
            ]
    both_cores = remote(
        staged.at[1 - core], inbox, inbox_send, inbox_recv, moved(s, PARTNER, 1), x
    )

    def chip_away(k):
        m = 7 * k
        z, y = chip // 4, lax.rem(chip, 4)
        return lax.rem(z + (m // 4) % 4, 4) * 4 + lax.rem(y + m % 4, 4)

    def give(k):
        owner = chip_away(k)
        return remote(
            staged.at[core, wide(owner, share_rows)], gathered.at[k],
            out_send.at[k], out_recv.at[k], owner * 2 + core, x,
        )

    stores[3].start()
    both_cores.start()
    dmerged = dot_nn(grad_resid[...], out_w[...])
    dconv[pl.ds(0, tokens), :] = dmerged * gate_b[...].astype(F32)
    grad_b[...] = (dmerged * conv[...]).astype(BF16)
    stores[5].start()
    both_cores.wait_recv()
    staged[core] = (staged[core].astype(F32) + inbox[...].astype(F32)).astype(BF16)

    @pl.when(s > 0)
    def _():
        sooner.start()

    @pl.when(s == 31)
    def _():
        dconv[pl.ds(tokens, EDGE), :] = jnp.zeros((EDGE, dconv.shape[1]), F32)

    gathered[0] = staged[core, wide(chip, share_rows), :]
    each(1, 16, lambda k: give(k).start())

    def finish(k):
        home(k).wait_send()

        @pl.when(k != PARTNER)
        def _():
            for h in range(2):
                near(h, k).wait_send()

    each(1, 32, finish)

    def finish_swap(k):
        for h in range(2):
            swap(h, k).wait_send()

    each(0, 32, finish_swap)
    other.wait_send()

    @pl.when(s < 31)
    def _():
        later.wait_send()
        sooner.wait_recv()

    dmixed = (
        taps[2:3, :] * dconv[pl.ds(0, tokens), :]
        + taps[1:2, :] * dconv[pl.ds(1, tokens), :]
        + taps[0:1, :] * dconv[pl.ds(2, tokens), :]
    )
    grad_c[...] = (dmixed * values[...].astype(F32)).astype(BF16)
    grad_values[...] = (dmixed * gate_c[...].astype(F32)).astype(BF16)
    each(1, 16, lambda k: give(k).wait_recv())
    for n in (6, 7):
        stores[n].start()
    grad_out[...] = jnp.sum(gathered[...].astype(F32), axis=0)
    each(1, 16, lambda k: give(k).wait_send())
    both_cores.wait_send()
    stores[4].start()
    for copy in stores:
        copy.wait()

    @pl.when(s > 0)
    def _():
        sooner.wait_send()


CUTS = (4, 4, 4, 3, 1, 1, 1, 1)


def hand_over_kernel(*refs):
    n = len(CUTS)
    sources, targets, held = refs[:n], refs[n : 2 * n], refs[2 * n : 3 * n]
    in_sem, out_sem = refs[3 * n :]
    into, out = [], []
    for i, cuts in enumerate(CUTS):
        rows = held[i].shape[0] // cuts
        for j in range(cuts):
            part = pl.ds(j * rows, rows)
            at = len(into)
            into.append(
                pltpu.make_async_copy(sources[i].at[part], held[i].at[part], in_sem.at[at])
            )
            out.append(
                pltpu.make_async_copy(held[i].at[part], targets[i].at[part], out_sem.at[at])
            )
    for copy in into:
        copy.start()
    for arriving, leaving in zip(into, out):
        arriving.wait()
        leaving.start()
    for copy in out:
        copy.wait()


def hand_over(arrays):
    anywhere = pl.BlockSpec(memory_space=pl.ANY)
    return pl.pallas_call(
        hand_over_kernel,
        out_shape=[jax.ShapeDtypeStruct(a.shape, a.dtype) for a in arrays],
        in_specs=[anywhere] * len(arrays),
        out_specs=[anywhere] * len(arrays),
        scratch_shapes=[pltpu.VMEM(a.shape, a.dtype) for a in arrays]
        + [pltpu.SemaphoreType.DMA((sum(CUTS),))] * 2,
        compiler_params=pltpu.CompilerParams(vmem_limit_bytes=60 * 2**20),
    )(*arrays)


def on_device(
    resid_in,
    cotangent,
    norm_gain,
    routes,
    route_weights,
    gate_weight,
    up_weight,
    down_weight,
    out_weight,
    gate_b,
    gate_c,
    values_u,
    taps,
):
    tokens, width = resid_in.shape
    hidden, channels = gate_weight.shape[2], gate_b.shape[1]
    experts = lax.axis_size("sp")
    slots = experts * SLOTS
    names = jnp.arange(experts, dtype=jnp.int32)[:, None]
    first, second = (routes[:, 0] == names).astype(F32), (routes[:, 1] == names).astype(F32)
    order = jnp.arange(tokens)
    ahead = jnp.dot(
        (first + second).astype(BF16),
        (order[:, None] < order[None, :]).astype(BF16),
        preferred_element_type=F32,
    )
    s = lax.axis_index("sp")
    slot = jnp.stack(
        [
            turn_of(routes[:, k], s) * SLOTS + jnp.sum(hit * ahead, axis=0).astype(jnp.int32)
            for k, hit in enumerate((first, second))
        ]
    )
    vmem = pl.BlockSpec(memory_space=pltpu.VMEM)
    dma = pltpu.SemaphoreType.DMA
    anywhere = pl.BlockSpec(memory_space=pl.ANY)
    results = [
            jax.ShapeDtypeStruct((width, hidden), F32),
            jax.ShapeDtypeStruct((width, hidden), F32),
            jax.ShapeDtypeStruct((hidden, width), F32),
            jax.ShapeDtypeStruct((tokens, width), BF16),
            jax.ShapeDtypeStruct((width // experts, channels), F32),
            jax.ShapeDtypeStruct((tokens, channels), BF16),
            jax.ShapeDtypeStruct((tokens, channels), BF16),
            jax.ShapeDtypeStruct((tokens, channels), BF16),
    ]
    outs = pl.pallas_call(
        experts_kernel,
        out_shape=results,
        in_specs=[vmem] * 10 + [anywhere] * 4,
        out_specs=[anywhere] * 8,
        scratch_shapes=[
            pltpu.VMEM((width, hidden), BF16),
            pltpu.VMEM((width, hidden), BF16),
            pltpu.VMEM((hidden, width), BF16),
            pltpu.VMEM((width, channels), BF16),
        ]
        + [pltpu.VMEM(r.shape, r.dtype) for r in results]
        + [dma((4,)), dma((8,))]
        + [
            pltpu.VMEM((2, slots, width), BF16),
            pltpu.VMEM((slots, width), BF16),
            pltpu.VMEM((SLOTS, width), BF16),
            pltpu.VMEM((slots, 1024), BF16),
            pltpu.VMEM((slots, 1024), BF16),
            pltpu.VMEM((2 * GROUP_ROWS, hidden), BF16),
            pltpu.VMEM((2 * GROUP_ROWS, hidden), BF16),
            pltpu.VMEM((2 * GROUP_ROWS, hidden), BF16),
            pltpu.VMEM((tokens, 512), BF16),
            pltpu.VMEM((tokens, 512), BF16),
            pltpu.VMEM((tokens, 512), F32),
            pltpu.VMEM((tokens, width), BF16),
            pltpu.VMEM((tokens, 128), F32),
            pltpu.VMEM((tokens, slots), BF16),
            pltpu.VMEM((tokens, width), BF16),
            pltpu.VMEM((tokens + EDGE, channels), F32),
            pltpu.VMEM((tokens, channels), F32),
            pltpu.VMEM((tokens, channels), BF16),
            pltpu.VMEM((tokens + EDGE, channels), F32),
            pltpu.VMEM((2, width // 2, channels), BF16),
            pltpu.VMEM((width // 2, channels), BF16),
            pltpu.VMEM((experts // 2, width // experts, channels), BF16),
        ]
        + [dma((32,)), dma((32,)), dma((2, 32)), dma((2, 32)), dma((2, 32)), dma((2, 32))]
        + [dma((32,))] * 2
        + [dma((16,))] * 2
        + [dma((6,))] * 2
        + [dma] * 10,
        compiler_params=pltpu.CompilerParams(
            collective_id=0, has_side_effects=True, vmem_limit_bytes=63 * 2**20
        ),
    )(
        resid_in, cotangent, norm_gain[None], slot, route_weights.T, slot.T,
        gate_b, gate_c, values_u, taps,
        gate_weight[0], up_weight[0], down_weight[0], out_weight,
    )
    outs = hand_over(outs)
    return (outs[0][None], outs[1][None], outs[2][None], *outs[3:])


def solution(mesh):
    placed = (
        P("sp", None),
        P("sp", None),
        P(),
        P("sp", None),
        P("sp", None),
        P("sp", None, "tp"),
        P("sp", None, "tp"),
        P("sp", "tp", None),
        P(None, "tp"),
        P("sp", "tp"),
        P("sp", "tp"),
        P("sp", "tp"),
        P(None, "tp"),
    )
    return jax.shard_map(
        on_device,
        mesh=mesh,
        in_specs=placed,
        out_specs=(
            P("sp", None, "tp"),
            P("sp", None, "tp"),
            P("sp", "tp", None),
            P("sp", None),
            P("sp", "tp"),
            P("sp", "tp"),
            P("sp", "tp"),
            P("sp", "tp"),
        ),
        check_vma=False,
    )
```

```python
import jax
import jax.numpy as jnp
from jax import lax
from jax.experimental import pallas as pl
from jax.experimental.pallas import tpu as pltpu
from jax.sharding import PartitionSpec as P

norm_eps = 1e-06


MESH = pl.DeviceIdType.MESH
BF16 = jnp.bfloat16
F32 = jnp.float32
SLOTS = 48
PER_GROUP = 4
GROUP_ROWS = PER_GROUP * SLOTS
GROUPS = 32 // PER_GROUP


def offsets(k):
    m = 13 * k
    return (m // 8) % 4, (m // 2) % 4, m % 2


def moved(s, k, sign):
    z, y, c = s // 8, (s // 2) % 4, s % 2
    dz, dy, dc = offsets(k)
    z = lax.rem(z + 4 + sign * dz, 4)
    y = lax.rem(y + 4 + sign * dy, 4)
    return (z * 4 + y) * 2 + lax.rem(c + dc, 2)


def turn_of(expert, s):
    dz = (expert // 8 - s // 8) % 4
    dy = ((expert // 2) % 4 - (s // 2) % 4) % 4
    dc = (expert - s) % 2
    return (5 * (dz * 8 + dy * 2 + dc)) % 32


def dot_nn(a, b):
    return jnp.dot(a, b, preferred_element_type=F32)


def dot_nt(a, b):
    return lax.dot_general(a, b, (((1,), (1,)), ((), ())), preferred_element_type=F32)


def dot_tn(a, b):
    return lax.dot_general(a, b, (((0,), (0,)), ((), ())), preferred_element_type=F32)


def block(k):
    return pl.ds(pl.multiple_of(k * SLOTS, SLOTS), SLOTS)


def group(g):
    return pl.ds(pl.multiple_of(g * GROUP_ROWS, GROUP_ROWS), GROUP_ROWS)


def wide(j, size):
    return pl.ds(pl.multiple_of(j * size, size), size)


PARTNER = 5
EARLY = 5
EDGE = 8


def experts_kernel(
    resid, cots, gain, slot, weight, slot_col, gate_b, gate_c, values, taps,
    gate_far, up_far, down_far, out_far,
    to_gate, to_up, to_down, to_resid, to_out, to_b, to_c, to_values,
    gate_w, up_w, down_w, out_w,
    grad_gate, grad_up, grad_down, grad_resid, grad_out, grad_b, grad_c, grad_values,
    load_sem, store_sem,
    both, part, extra, swapped, back, hidden, dgate, dup, half_out, half_in, half_own,
    normed, inverse, pick, total, mixed, conv, merged, dconv, staged, inbox, gathered,
    far_send, far_recv, near_send, near_recv, swap_send, swap_recv, back_send, back_recv,
    out_send, out_recv, all_send, all_recv,
    extra_send, extra_recv, half_send, half_recv, later_send, later_recv, sooner_send, sooner_recv,
    inbox_send, inbox_recv,
):
    s, x = lax.axis_index("sp"), lax.axis_index("tp")
    kind = lax.rem(x, 2)
    high = x // 2
    right, left, across = lax.rem(x + 1, 4), lax.rem(x + 3, 4), lax.rem(x + 2, 4)
    sides = (right, left)
    given = (1 + 2 * kind, 2 - 2 * kind)
    kept = (2 * kind, 3 - 2 * kind)
    tokens = cots.shape[0]
    barrier = pltpu.get_barrier_semaphore()

    def each(first, last, action):
        def body(k, carry):
            action(k)
            return carry

        lax.fori_loop(first, last, body, 0)

    def greet(k):
        pl.semaphore_signal(
            barrier, inc=1, device_id={"sp": moved(s, k, 1), "tp": x}, device_id_type=MESH
        )

    loads = [
        pltpu.make_async_copy(source, target, load_sem.at[i])
        for i, (source, target) in enumerate(
            ((gate_far, gate_w), (up_far, up_w), (down_far, down_w), (out_far, out_w))
        )
    ]
    stores = [
        pltpu.make_async_copy(source, target, store_sem.at[i])
        for i, (source, target) in enumerate(
            (
                (grad_gate, to_gate), (grad_up, to_up), (grad_down, to_down),
                (grad_resid, to_resid), (grad_out, to_out), (grad_b, to_b),
                (grad_c, to_c), (grad_values, to_values),
            )
        )
    ]
    each(1, 32, greet)
    for lane in (right, left, across):
        pl.semaphore_signal(barrier, inc=1, device_id={"sp": s, "tp": lane}, device_id_type=MESH)

    def remote(source, target, sent, received, sp, tp):
        return pltpu.make_async_remote_copy(
            src_ref=source,
            dst_ref=target,
            send_sem=sent,
            recv_sem=received,
            device_id={"sp": sp, "tp": tp},
            device_id_type=MESH,
        )

    def far(k):
        return remote(
            part.at[block(k)], both.at[kind, block(k)], far_send.at[k], far_recv.at[k],
            moved(s, k, 1), x,
        )

    def near(h, k):
        piece = both.at[kind, block(k), pl.ds(h * 1024, 1024)]
        return remote(piece, piece, near_send.at[h, k], near_recv.at[h, k], s, sides[h])

    def swap(h, k):
        return remote(
            part.at[block(k), wide(given[h], 512)],
            swapped.at[block(k), pl.ds((1 - h) * 512, 512)],
            swap_send.at[h, k], swap_recv.at[h, k], s, sides[h],
        )

    def home(k):
        return remote(
            swapped.at[block(k)], back.at[block(k)], back_send.at[k], back_recv.at[k],
            moved(s, k, -1), x,
        )

    other = remote(
        extra, both.at[1 - kind, block(PARTNER)], extra_send, extra_recv, moved(s, PARTNER, 1), x
    )
    later = remote(
        mixed.at[pl.ds(tokens, EDGE)], mixed.at[pl.ds(0, EDGE)], later_send, later_recv,
        jnp.minimum(s + 1, 31), x,
    )
    sooner = remote(
        dconv.at[pl.ds(0, EDGE)], dconv.at[pl.ds(tokens, EDGE)], sooner_send, sooner_recv,
        jnp.maximum(s - 1, 0), x,
    )

    def normalize(i):
        rows = wide(i, 64)
        held = resid[rows, :].astype(F32)
        scale = lax.rsqrt(jnp.mean(held * held, axis=1, keepdims=True) + norm_eps)
        normed[rows, :] = (held * scale * gain[...]).astype(BF16)
        inverse[rows, :] = jnp.broadcast_to(scale, (64, 128))

    for copy in loads:
        copy.start()
    each(0, tokens // 64, normalize)

    def pack(target, rows, first, count, is_cot):
        ids = lax.broadcasted_iota(jnp.int32, (count * SLOTS, tokens), 0) + first * SLOTS
        zero = jnp.zeros((count * SLOTS, tokens), F32)
        ones = jnp.ones((1, tokens), F32)
        value = [weight[k : k + 1, :] if is_cot else ones for k in range(2)]
        chosen = jnp.where(
            ids == slot[0:1, :], value[0], jnp.where(ids == slot[1:2, :], value[1], zero)
        ).astype(BF16)
        data = cots if is_cot else normed
        for j in range(4):
            cols = pl.ds(j * 512, 512)
            target[rows, cols] = dot_nn(chosen, data[:, cols]).astype(BF16)

    def pack_group(g):
        for option in range(2):

            @pl.when(kind == option)
            def _():
                rows = wide(g, 4 * SLOTS)
                pack(part, rows, g * 4, 4, option == 1)

    pack_group(0)
    mixed[pl.ds(EDGE, tokens), :] = gate_c[...].astype(F32) * values[...].astype(F32)
    pl.semaphore_wait(barrier, 34)

    def pass_on(k):
        far(k).wait_recv()

        @pl.when(k != PARTNER)
        def _():
            for h in range(2):
                near(h, k).start()

    def pack_and_send(g, carry):
        pack_group(g)
        each(jnp.maximum(g * 4 - 4, 1), g * 4, lambda k: far(k).start())

        @pl.when(g >= 4)
        def _():
            pass_on(g - 3)

        return carry

    lax.fori_loop(1, 8, pack_and_send, 0)
    each(28, 32, lambda k: far(k).start())

    @pl.when(s < 31)
    def _():
        later.start()

    for option in range(2):
        pack(both.at[option], pl.ds(0, SLOTS), 0, 1, option == 1)

        @pl.when(kind == option)
        def _():
            pack(extra, pl.ds(0, SLOTS), PARTNER, 1, option == 0)

    def arrived(k):
        @pl.when((k != PARTNER) & (k != 0))
        def _():
            for h in range(2):
                near(h, k).wait_recv()

        @pl.when(k == PARTNER)
        def _():
            other.wait_recv()

    def expert(g):
        rows = group(g)
        local = wide(lax.rem(g, 2), GROUP_ROWS)
        row, cot = both[0, rows, :], both[1, rows, :]
        gate = dot_nn(row, gate_w[...])
        up = dot_nn(row, up_w[...])
        dhidden = dot_nt(cot, down_w[...])
        logistic = jax.nn.sigmoid(gate)
        activated = gate * logistic
        hidden[local, :] = (activated * up).astype(BF16)
        dgate[local, :] = (dhidden * up * logistic * (1.0 + gate * (1.0 - logistic))).astype(BF16)
        dup[local, :] = (dhidden * activated).astype(BF16)

        def tile(j):
            cols = wide(j, 512)
            part[rows, cols] = (
                dot_nt(dgate[local, :], gate_w[cols, :]) + dot_nt(dup[local, :], up_w[cols, :])
            ).astype(BF16)

        each(0, 4, tile)

    def weights(chunk):
        rows = wide(chunk, 2 * GROUP_ROWS)

        def tile(j):
            cols = wide(j, 512)
            row = both[0, rows, cols]
            grad_gate[cols, :] += dot_tn(row, dgate[...])
            grad_up[cols, :] += dot_tn(row, dup[...])
            grad_down[:, cols] += dot_tn(hidden[...], both[1, rows, cols])

        each(0, 4, tile)

    def swap_arrived(k):
        for h in range(2):
            swap(h, k).wait_recv()

    def pair_sum(g):
        rows = group(g)
        for h in range(2):
            cols = pl.ds(h * 512, 512)
            swapped[rows, cols] = (
                part[rows, wide(kept[h], 512)].astype(F32) + swapped[rows, cols].astype(F32)
            ).astype(BF16)

    def make_pick():
        ids = lax.broadcasted_iota(jnp.int32, pick.shape, 1)
        hit = (ids == slot_col[:, 0:1]) | (ids == slot_col[:, 1:2])
        pick[...] = jnp.where(hit, 1.0, 0.0).astype(BF16)

    def make_conv():
        @pl.when(s == 0)
        def _():
            mixed[pl.ds(0, EDGE), :] = jnp.zeros((EDGE, mixed.shape[1]), F32)

        @pl.when(s > 0)
        def _():
            later.wait_recv()

        conv[...] = (
            taps[0:1, :] * mixed[pl.ds(EDGE - 2, tokens), :]
            + taps[1:2, :] * mixed[pl.ds(EDGE - 1, tokens), :]
            + taps[2:3, :] * mixed[pl.ds(EDGE, tokens), :]
        )
        merged[...] = (gate_b[...].astype(F32) * conv[...]).astype(BF16)

    def step(g, carry):
        first = g * PER_GROUP

        @pl.when(g < GROUPS)
        def _():
            each(jnp.maximum(first, EARLY), first + PER_GROUP // 2, pass_on)

        @pl.when(g == 0)
        def _():
            other.start()
            for copy in loads:
                copy.wait()
            grad_gate[...] = jnp.zeros_like(grad_gate)
            grad_up[...] = jnp.zeros_like(grad_up)
            grad_down[...] = jnp.zeros_like(grad_down)

        @pl.when((g >= 1) & (g <= GROUPS))
        def _():
            each(first - PER_GROUP, first, arrived)
            each(jnp.maximum(first - PER_GROUP, 1), first, lambda k: far(k).wait_send())
            expert(g - 1)

        @pl.when((g >= 2) & (g <= GROUPS + 1))
        def _():
            each(first - 2 * PER_GROUP, first - PER_GROUP, swap_arrived)
            pair_sum(g - 2)

        @pl.when((g >= 1) & (g <= GROUPS))
        def _():
            def send(k):
                for h in range(2):
                    swap(h, k).start()

            each(first - PER_GROUP, first, send)

        @pl.when((g >= 2) & (g <= GROUPS + 1))
        def _():
            each(jnp.maximum(first - 2 * PER_GROUP, 1), first - PER_GROUP, lambda k: home(k).start())

        @pl.when(g < GROUPS)
        def _():
            each(jnp.maximum(first + PER_GROUP // 2, EARLY), first + PER_GROUP, pass_on)

        @pl.when((g >= 2) & (g < GROUPS) & (lax.rem(g, 2) == 0))
        def _():
            weights(g // 2 - 1)

        @pl.when(g == 3)
        def _():
            make_pick()

        @pl.when(g == 5)
        def _():
            make_conv()

        return carry

    lax.fori_loop(0, GROUPS + 2, step, 0)
    back[block(0), :] = swapped[block(0), :]
    weights(GROUPS // 2 - 1)
    each(1, 32, lambda k: home(k).wait_recv())
    for copy in stores[:3]:
        copy.start()

    def summed(half, j):
        return dot_nn(pick[...], back[:, wide(half * 2 + j, 256)])

    for j in range(2):
        half_out[:, pl.ds(j * 256, 256)] = summed(1 - high, j).astype(BF16)
    cross = remote(half_out, half_in, half_send, half_recv, s, across)
    cross.start()
    for j in range(2):
        half_own[:, pl.ds(j * 256, 256)] = summed(high, j)
    cross.wait()

    def quarter_of(lane):
        odd, upper = lax.rem(lane, 2), lane // 2
        return (1 - upper) * 2 * odd + upper * (3 - 2 * odd)

    total[:, wide(quarter_of(x), 512)] = (half_own[...] + half_in[...].astype(F32)).astype(BF16)

    def share(n, owner, h, lane):
        piece = total.at[pl.ds(h * (tokens // 2), tokens // 2), wide(quarter_of(owner), 512)]
        return remote(piece, piece, all_send.at[n], all_recv.at[n], s, lane)

    shares = [
        share(0, x, 0, right),
        share(1, x, 1, right),
        share(2, x, 0, left),
        share(3, x, 1, left),
        share(4, left, 0, right),
        share(5, right, 1, left),
    ]
    for n in (0, 3, 1, 2):
        shares[n].start()
    shares[0].wait_recv()
    shares[4].start()
    shares[3].wait_recv()
    shares[5].start()
    for n in (1, 2, 4, 5):
        shares[n].wait_recv()
    for copy in shares:
        copy.wait_send()

    def resid_tile(i):
        rows = wide(i, 64)
        scaled = total[rows, :].astype(F32) * gain[...]
        held = resid[rows, :].astype(F32)
        scale = inverse[rows, 0:1]
        mean = jnp.mean(scaled * held, axis=1, keepdims=True)
        grad_resid[rows, :] = (
            cots[rows, :].astype(F32) + scale * scaled - held * (scale * scale * scale * mean)
        ).astype(BF16)

    each(0, tokens // 64, resid_tile)
    share_rows = grad_out.shape[0]
    core, chip = lax.rem(s, 2), s // 2
    for j in range(4):
        cols = pl.ds(j * 512, 512)
        piece = dot_tn(grad_resid[:, cols], merged[...]).astype(BF16)
        for i in range(8):
            staged[i % 2, pl.ds((j * 4 + i // 2) * share_rows, share_rows), :] = piece[
                i * share_rows : (i + 1) * share_rows
            ]
    both_cores = remote(
        staged.at[1 - core], inbox, inbox_send, inbox_recv, moved(s, PARTNER, 1), x
    )

    def chip_away(k):
        m = 7 * k
        z, y = chip // 4, lax.rem(chip, 4)
        return lax.rem(z + (m // 4) % 4, 4) * 4 + lax.rem(y + m % 4, 4)

    def give(k):
        owner = chip_away(k)
        return remote(
            staged.at[core, wide(owner, share_rows)], gathered.at[k],
            out_send.at[k], out_recv.at[k], owner * 2 + core, x,
        )

    stores[3].start()
    both_cores.start()
    dmerged = dot_nn(grad_resid[...], out_w[...])
    dconv[pl.ds(0, tokens), :] = dmerged * gate_b[...].astype(F32)
    grad_b[...] = (dmerged * conv[...]).astype(BF16)
    stores[5].start()
    both_cores.wait_recv()
    staged[core] = (staged[core].astype(F32) + inbox[...].astype(F32)).astype(BF16)

    @pl.when(s > 0)
    def _():
        sooner.start()

    @pl.when(s == 31)
    def _():
        dconv[pl.ds(tokens, EDGE), :] = jnp.zeros((EDGE, dconv.shape[1]), F32)

    gathered[0] = staged[core, wide(chip, share_rows), :]
    each(1, 16, lambda k: give(k).start())

    def finish(k):
        home(k).wait_send()

        @pl.when(k != PARTNER)
        def _():
            for h in range(2):
                near(h, k).wait_send()

    each(1, 32, finish)

    def finish_swap(k):
        for h in range(2):
            swap(h, k).wait_send()

    each(0, 32, finish_swap)
    other.wait_send()

    @pl.when(s < 31)
    def _():
        later.wait_send()
        sooner.wait_recv()

    dmixed = (
        taps[2:3, :] * dconv[pl.ds(0, tokens), :]
        + taps[1:2, :] * dconv[pl.ds(1, tokens), :]
        + taps[0:1, :] * dconv[pl.ds(2, tokens), :]
    )
    grad_c[...] = (dmixed * values[...].astype(F32)).astype(BF16)
    grad_values[...] = (dmixed * gate_c[...].astype(F32)).astype(BF16)
    each(1, 16, lambda k: give(k).wait_recv())
    for n in (6, 7):
        stores[n].start()
    grad_out[...] = jnp.sum(gathered[...].astype(F32), axis=0)
    each(1, 16, lambda k: give(k).wait_send())
    both_cores.wait_send()
    stores[4].start()
    for copy in stores:
        copy.wait()

    @pl.when(s > 0)
    def _():
        sooner.wait_send()


CUTS = (4, 4, 4, 3, 1, 1, 1, 1)


def hand_over_kernel(*refs):
    n = len(CUTS)
    sources, targets, held = refs[:n], refs[n : 2 * n], refs[2 * n : 3 * n]
    in_sem, out_sem = refs[3 * n :]
    into, out = [], []
    for i, cuts in enumerate(CUTS):
        rows = held[i].shape[0] // cuts
        for j in range(cuts):
            part = pl.ds(j * rows, rows)
            at = len(into)
            into.append(
                pltpu.make_async_copy(sources[i].at[part], held[i].at[part], in_sem.at[at])
            )
            out.append(
                pltpu.make_async_copy(held[i].at[part], targets[i].at[part], out_sem.at[at])
            )
    for copy in into:
        copy.start()
    for arriving, leaving in zip(into, out):
        arriving.wait()
        leaving.start()
    for copy in out:
        copy.wait()


def hand_over(arrays):
    anywhere = pl.BlockSpec(memory_space=pl.ANY)
    return pl.pallas_call(
        hand_over_kernel,
        out_shape=[jax.ShapeDtypeStruct(a.shape, a.dtype) for a in arrays],
        in_specs=[anywhere] * len(arrays),
        out_specs=[anywhere] * len(arrays),
        scratch_shapes=[pltpu.VMEM(a.shape, a.dtype) for a in arrays]
        + [pltpu.SemaphoreType.DMA((sum(CUTS),))] * 2,
        compiler_params=pltpu.CompilerParams(vmem_limit_bytes=60 * 2**20),
    )(*arrays)


def on_device(
    resid_in,
    cotangent,
    norm_gain,
    routes,
    route_weights,
    gate_weight,
    up_weight,
    down_weight,
    out_weight,
    gate_b,
    gate_c,
    values_u,
    taps,
):
    tokens, width = resid_in.shape
    hidden, channels = gate_weight.shape[2], gate_b.shape[1]
    experts = lax.axis_size("sp")
    slots = experts * SLOTS
    names = jnp.arange(experts, dtype=jnp.int32)[:, None]
    first, second = (routes[:, 0] == names).astype(F32), (routes[:, 1] == names).astype(F32)
    order = jnp.arange(tokens)
    ahead = jnp.dot(
        (first + second).astype(BF16),
        (order[:, None] < order[None, :]).astype(BF16),
        preferred_element_type=F32,
    )
    s = lax.axis_index("sp")
    slot = jnp.stack(
        [
            turn_of(routes[:, k], s) * SLOTS + jnp.sum(hit * ahead, axis=0).astype(jnp.int32)
            for k, hit in enumerate((first, second))
        ]
    )
    vmem = pl.BlockSpec(memory_space=pltpu.VMEM)
    dma = pltpu.SemaphoreType.DMA
    anywhere = pl.BlockSpec(memory_space=pl.ANY)
    results = [
            jax.ShapeDtypeStruct((width, hidden), F32),
            jax.ShapeDtypeStruct((width, hidden), F32),
            jax.ShapeDtypeStruct((hidden, width), F32),
            jax.ShapeDtypeStruct((tokens, width), BF16),
            jax.ShapeDtypeStruct((width // experts, channels), F32),
            jax.ShapeDtypeStruct((tokens, channels), BF16),
            jax.ShapeDtypeStruct((tokens, channels), BF16),
            jax.ShapeDtypeStruct((tokens, channels), BF16),
    ]
    outs = pl.pallas_call(
        experts_kernel,
        out_shape=results,
        in_specs=[vmem] * 10 + [anywhere] * 4,
        out_specs=[anywhere] * 8,
        scratch_shapes=[
            pltpu.VMEM((width, hidden), BF16),
            pltpu.VMEM((width, hidden), BF16),
            pltpu.VMEM((hidden, width), BF16),
            pltpu.VMEM((width, channels), BF16),
        ]
        + [pltpu.VMEM(r.shape, r.dtype) for r in results]
        + [dma((4,)), dma((8,))]
        + [
            pltpu.VMEM((2, slots, width), BF16),
            pltpu.VMEM((slots, width), BF16),
            pltpu.VMEM((SLOTS, width), BF16),
            pltpu.VMEM((slots, 1024), BF16),
            pltpu.VMEM((slots, 1024), BF16),
            pltpu.VMEM((2 * GROUP_ROWS, hidden), BF16),
            pltpu.VMEM((2 * GROUP_ROWS, hidden), BF16),
            pltpu.VMEM((2 * GROUP_ROWS, hidden), BF16),
            pltpu.VMEM((tokens, 512), BF16),
            pltpu.VMEM((tokens, 512), BF16),
            pltpu.VMEM((tokens, 512), F32),
            pltpu.VMEM((tokens, width), BF16),
            pltpu.VMEM((tokens, 128), F32),
            pltpu.VMEM((tokens, slots), BF16),
            pltpu.VMEM((tokens, width), BF16),
            pltpu.VMEM((tokens + EDGE, channels), F32),
            pltpu.VMEM((tokens, channels), F32),
            pltpu.VMEM((tokens, channels), BF16),
            pltpu.VMEM((tokens + EDGE, channels), F32),
            pltpu.VMEM((2, width // 2, channels), BF16),
            pltpu.VMEM((width // 2, channels), BF16),
            pltpu.VMEM((experts // 2, width // experts, channels), BF16),
        ]
        + [dma((32,)), dma((32,)), dma((2, 32)), dma((2, 32)), dma((2, 32)), dma((2, 32))]
        + [dma((32,))] * 2
        + [dma((16,))] * 2
        + [dma((6,))] * 2
        + [dma] * 10,
        compiler_params=pltpu.CompilerParams(
            collective_id=0, has_side_effects=True, vmem_limit_bytes=63 * 2**20
        ),
    )(
        resid_in, cotangent, norm_gain[None], slot, route_weights.T, slot.T,
        gate_b, gate_c, values_u, taps,
        gate_weight[0], up_weight[0], down_weight[0], out_weight,
    )
    outs = hand_over(outs)
    return (outs[0][None], outs[1][None], outs[2][None], *outs[3:])


def solution(mesh):
    placed = (
        P("sp", None),
        P("sp", None),
        P(),
        P("sp", None),
        P("sp", None),
        P("sp", None, "tp"),
        P("sp", None, "tp"),
        P("sp", "tp", None),
        P(None, "tp"),
        P("sp", "tp"),
        P("sp", "tp"),
        P("sp", "tp"),
        P(None, "tp"),
    )
    return jax.shard_map(
        on_device,
        mesh=mesh,
        in_specs=placed,
        out_specs=(
            P("sp", None, "tp"),
            P("sp", None, "tp"),
            P("sp", "tp", None),
            P("sp", None),
            P("sp", "tp"),
            P("sp", "tp"),
            P("sp", "tp"),
            P("sp", "tp"),
        ),
        check_vma=False,
    )
```
